128 devices in a mesh: sp: 32 (over z, y, core), tp: 4 (over x).
Axes of the slice: x: 4, y: 4, z: 4, core: 2. Of those that a mesh axis runs over, the one named last changes fastest.
Arguments:
- queries: bfloat16 [16384, 2048], P('sp', 'tp'), may hold values from -8 to 8
- keys: bfloat16 [16384, 512], P('sp', 'tp'), may hold values from -8 to 8
- values: bfloat16 [16384, 512], P('sp', 'tp'), may hold values from -6 to 6
- q_gain: float32 [128], replicated, may hold values from 0.1 to 5.8
- k_gain: float32 [128], replicated, may hold values from 0.1 to 5.8
- out_weight: bfloat16 [2048, 2048], replicated, may hold values from -0.125 to 0.125
- out_gain: float32 [2048], replicated, may hold values from 0.1 to 1.9
- residual_in: bfloat16 [16384, 2048], P(('sp', 'tp')), may hold values from -6 to 6
- mlp_gain: float32 [2048], replicated, may hold values from 0.1 to 1.9
- gate_weight: bfloat16 [2048, 5632], P('sp', 'tp'), may hold values from -0.125 to 0.125
- up_weight: bfloat16 [2048, 5632], P('sp', 'tp'), may hold values from -0.125 to 0.125
- down_weight: bfloat16 [5632, 2048], P('tp', 'sp'), may hold values from -0.078125 to 0.078125
- final_gain: float32 [2048], replicated, may hold values from 0.1 to 1.9
Outputs:
- layer_out: bfloat16 [16384, 2048], P(('sp', 'tp'))
The draws below stay inside these ranges and needn't reach their ends.
All inputs are finite; a program needn't handle non-finite values.
Results may differ from the reference program's by a relative error of at most 0.015.
The reference program's roundings to bfloat16 on the way count: a program that leaves them out, or rounds other values in their place, can miss the bound.
Values may be sent and summed in bfloat16 or wider, within the bound.
A program may use at most 128 MiB of HBM per device.

```python
import jax
import jax.numpy as jnp
from jax import lax

D = 2048
HQ = 16
KV = 4
HD = 128
FF = 5632
GRID_W = 64
TOK_DEV = 512
TOKENS = 16384


def drawn(base_key):
    query_base = jnp.clip(jax.random.normal(jax.random.fold_in(base_key, 101), (TOKENS, HQ, HD), jnp.float32), -6.0, 6.0)
    key_base = jnp.clip(jax.random.normal(jax.random.fold_in(base_key, 102), (TOKENS, KV, HD), jnp.float32), -6.0, 6.0)
    return (query_base.reshape(TOKENS, HQ * HD), key_base.reshape(TOKENS, KV * HD))


def gain_values(base_key):
    return 1.0 + 0.18 * jnp.clip(jax.random.normal(base_key, (HD,), jnp.float32), -5.0, 5.0)


def draw_queries(key, part):
    return drawn(key)[0].astype(jnp.bfloat16)


def draw_keys(key, part):
    return drawn(key)[1].astype(jnp.bfloat16)


def draw_q_gain(key, part):
    return gain_values(jax.random.fold_in(key, 201))


def draw_k_gain(key, part):
    return gain_values(jax.random.fold_in(key, 202))


def level_of(own_key, shape, shards, smallest, largest):
    gain, own = 1.0, jax.random.fold_in(own_key, 6)
    for position, shards_of in shards:
        draws = jnp.exp(jax.random.uniform(jax.random.fold_in(own, position), (shards_of,), jnp.float32, smallest / len(shards), largest / len(shards)))
        gain = gain * jnp.repeat(draws, shape[position] // shards_of).reshape([-1 if axis == position else 1 for axis in range(len(shape))])
    return gain


def scatter_about(key, extent, spread, bound, shards=(), kind=jnp.bfloat16):
    loudness = level_of(key, extent, shards, -0.22, 0.18) if shards else 1.0
    entries = jax.random.normal(key, extent, jnp.float32) * spread * loudness
    return jnp.minimum(jnp.maximum(entries, -bound), bound).astype(kind)


def setup_inputs(seed: int = 0) -> dict:
    splits = jax.random.split(jax.random.key(seed), 14)
    queries = draw_queries(jax.random.fold_in(splits[13], 71), 0)
    keys = draw_keys(jax.random.fold_in(splits[13], 71), 0)
    values = scatter_about(splits[2], (TOKENS, KV * HD), 1.0, 6.0, ((0, 32), (1, 4)))
    q_gain = draw_q_gain(jax.random.fold_in(splits[13], 71), 0)
    k_gain = draw_k_gain(jax.random.fold_in(splits[13], 71), 0)
    out_weight = scatter_about(splits[5], (HQ * HD, D), (HQ * HD) ** -0.5, 0.125)
    out_gain = jnp.clip(1.0 + 0.18 * jax.random.normal(splits[6], (D,), jnp.float32), 0.1, 1.9)
    residual_in = scatter_about(splits[7], (TOKENS, D), 1.0, 6.0, ((0, 128),))
    mlp_gain = jnp.clip(1.0 + 0.18 * jax.random.normal(splits[8], (D,), jnp.float32), 0.1, 1.9)
    gate_weight = scatter_about(splits[9], (D, FF), D ** -0.5, 0.125, ((0, 32), (1, 4)))
    up_weight = scatter_about(splits[10], (D, FF), D ** -0.5, 0.125, ((0, 32), (1, 4)))
    down_weight = scatter_about(splits[11], (FF, D), FF ** -0.5, 0.078125, ((0, 4), (1, 32)))
    final_gain = jnp.clip(1.0 + 0.18 * jax.random.normal(splits[12], (D,), jnp.float32), 0.1, 1.9)
    return dict(queries=queries, keys=keys, values=values, q_gain=q_gain, k_gain=k_gain, out_weight=out_weight, out_gain=out_gain, residual_in=residual_in, mlp_gain=mlp_gain, gate_weight=gate_weight, up_weight=up_weight, down_weight=down_weight, final_gain=final_gain)


def rms_scale(matrix):
    return matrix * lax.rsqrt(lax.optimization_barrier(jnp.mean(matrix * matrix, axis=-1, keepdims=True)) + 1e-06)

def rotary(matrix, positions):
    quarter = matrix.shape[-1] // 4
    freqs = 10000.0 ** (-jnp.arange(quarter, dtype=jnp.float32) / quarter)
    grid = jnp.stack([positions // GRID_W, positions % GRID_W], axis=-1).astype(jnp.float32)
    angle = grid[:, :, None] * freqs
    cosine = jnp.cos(angle)[:, None]
    sine = jnp.sin(angle)[:, None]
    parts = matrix.reshape(matrix.shape[:-1] + (2, 2, quarter))
    first = parts[..., 0, :]
    second = parts[..., 1, :]
    turned = jnp.stack([first * cosine - second * sine, second * cosine + first * sine], axis=-2)
    return turned.reshape(matrix.shape)

def reference(queries, keys, values, q_gain, k_gain, out_weight, out_gain, residual_in, mlp_gain, gate_weight, up_weight, down_weight, final_gain):
    tok_total = queries.shape[0]
    positions = jnp.arange(tok_total, dtype=jnp.int32)
    query_rot = rotary(rms_scale(queries.reshape(tok_total, HQ, HD).astype(jnp.float32)) * q_gain, positions).astype(jnp.bfloat16)
    key_rot = rotary(rms_scale(keys.reshape(tok_total, KV, HD).astype(jnp.float32)) * k_gain, positions).astype(jnp.bfloat16)
    value_heads = values.reshape(tok_total, KV, HD)
    group_size = HQ // KV
    score_scale = HD ** (-0.5)

    def one_head(head_index):
        query_head = lax.dynamic_index_in_dim(query_rot, head_index, 1, keepdims=False)
        key_head = lax.dynamic_index_in_dim(key_rot, head_index // group_size, 1, keepdims=False)
        value_head = lax.dynamic_index_in_dim(value_heads, head_index // group_size, 1, keepdims=False)

        def one_block(query_block):
            scores = jnp.dot(query_block, key_head.T, preferred_element_type=jnp.float32) * score_scale
            highest = lax.optimization_barrier(jnp.max(scores, axis=-1, keepdims=True))
            exp_scores = jnp.exp(scores - highest)
            weight_sum = lax.optimization_barrier(jnp.sum(exp_scores, axis=-1, keepdims=True))
            mixed = jnp.dot(exp_scores.astype(jnp.bfloat16), value_head, preferred_element_type=jnp.float32) / weight_sum
            return mixed.astype(jnp.bfloat16)
        blocks = query_head.reshape(tok_total // TOK_DEV, TOK_DEV, HD)
        return lax.map(one_block, blocks).reshape(tok_total, HD)
    per_head = lax.map(one_head, jnp.arange(HQ, dtype=jnp.int32))
    attended = jnp.transpose(per_head, (1, 0, 2)).reshape(tok_total, HQ * HD)
    projected = jnp.dot(attended, out_weight, preferred_element_type=jnp.float32)
    mid_stream = (residual_in.astype(jnp.float32) + out_gain * rms_scale(projected)).astype(jnp.bfloat16)
    normed = (mlp_gain * rms_scale(mid_stream.astype(jnp.float32))).astype(jnp.bfloat16)
    gate_proj = jnp.dot(normed, gate_weight, preferred_element_type=jnp.float32)
    up_proj = jnp.dot(normed, up_weight, preferred_element_type=jnp.float32)
    hidden = (jax.nn.silu(gate_proj) * up_proj).astype(jnp.bfloat16)
    mlp_branch = jnp.dot(hidden, down_weight, preferred_element_type=jnp.float32)
    return (mid_stream.astype(jnp.float32) + final_gain * rms_scale(mlp_branch)).astype(jnp.bfloat16)
```

```python
import functools
import math

import jax
import jax.numpy as jnp
from jax import lax
from jax.experimental import pallas as pl
from jax.experimental.pallas import tpu as pltpu
from jax.sharding import PartitionSpec as P

GRID_W = 64
MESH = pl.DeviceIdType.MESH
EPS = 1e-06
LOG2_SCALE = 128 ** (-0.5) * math.log2(math.e)
UNIT = 512
PHASE1 = 10

RING = [
    ("A", 1, (0, 0), None, (-1, 0)),
    ("A", -1, (0, 0), None, (1, 0)),
    ("B", 1, (0, 0), None, (0, -1)),
    ("B", -1, (0, 0), None, (0, 1)),
    ("A", 1, (-1, 0), 0, (2, 0)),
    ("A", -1, (1, 0), 1, (2, 0)),
    ("B", 1, (-1, 0), None, (-1, -1)),
    ("B", -1, (-1, 0), None, (-1, 1)),
    ("B", 1, (1, 0), None, (1, -1)),
    ("B", -1, (1, 0), None, (1, 1)),
    ("B", 1, (0, -1), 0, (0, 2)),
    ("B", -1, (0, 1), 1, (0, 2)),
    ("B", 1, (2, 0), None, (2, -1)),
    ("B", -1, (2, 0), None, (2, 1)),
    ("B", 1, (-1, -1), 0, (-1, 2)),
    ("B", -1, (-1, 1), 1, (-1, 2)),
    ("B", 1, (1, -1), 0, (1, 2)),
    ("B", -1, (1, 1), 1, (1, 2)),
    ("B", 1, (2, -1), 0, (2, 2)),
    ("B", -1, (2, 1), 1, (2, 2)),
]
PLACES = [(0, 0), (-1, 0), (1, 0), (0, -1), (0, 1), (2, 0), (0, 2), (-1, -1), (-1, 1), (1, -1), (1, 1), (2, -1), (2, 1), (-1, 2), (1, 2), (2, 2)]
STAGES = [
    ([], [0, 1, 2, 3], [(0, 0)]),
    ([0, 1, 2, 3], [4, 5, 10, 11, 6, 7, 8, 9], [(-1, 0), (1, 0), (0, -1), (0, 1)]),
    ([4, 5, 10, 11, 6, 7, 8, 9], [12, 13, 14, 15, 16, 17], [(2, 0), (0, 2), (-1, -1), (-1, 1), (1, -1), (1, 1)]),
    ([12, 13, 14, 15, 16, 17], [18, 19], [(2, -1), (2, 1), (-1, 2), (1, 2)]),
    ([18, 19], [], [(2, 2)]),
]
OWN_SLOT = {(0, 0): 0, (-1, 0): 2, (1, 0): 3, (0, -1): 4, (0, 1): 5, (2, 0): 10, (0, 2): 11, (-1, -1): 12, (-1, 1): 13, (1, -1): 14, (1, 1): 15,
            (2, -1): 22, (2, 1): 23, (-1, 2): 24, (1, 2): 25, (2, 2): 30}
PARTNER_SLOT = {(0, 0): 1, (-1, 0): 6, (1, 0): 7, (0, -1): 8, (0, 1): 9, (2, 0): 16, (0, 2): 17, (-1, -1): 18, (-1, 1): 19, (1, -1): 20, (1, 1): 21,
                (2, -1): 26, (2, 1): 27, (-1, 2): 28, (1, 2): 29, (2, 2): 31}
N_COPIES = len(RING) + len(PLACES)


def normalized(x):
    return x * lax.rsqrt(jnp.mean(x * x, axis=-1, keepdims=True) + EPS)


def layer_kernel(n, tp, q_ref, k_ref, v_ref, cos_ref, sin_ref, qg_ref, kg_ref, og_ref, mg_ref, fg_ref,
                 ow_hbm, res_hbm, gate_hbm, up_hbm, down_hbm, out_ref,
                 kv, gu, dt, ow, res, att, mid, nrm, hid, part, recv, proj, qt, s0, s1, acc, m_ref, l_ref,
                 send_sem, recv_sem, x_send, x_recv, local_sem):
    a = lax.axis_index("sp")
    t = lax.axis_index("tp")
    c = lax.rem(a, 2)
    chip = lax.div(a, 2)
    z = lax.div(chip, n)
    y = lax.rem(chip, n)
    u = y * (1 - c) + z * c
    w = z * (1 - c) + y * c
    partner = a + 1 - 2 * c

    def device_at(uu, ww, cc):
        return ((ww * (1 - cc) + uu * cc) * n + uu * (1 - cc) + ww * cc) * 2 + cc

    def own_index(du, dw):
        return device_at(lax.rem(u + du + n, n), lax.rem(w + dw + n, n), c)

    def partner_index(du, dw):
        return device_at(lax.rem(w + du + n, n), lax.rem(u + dw + n, n), 1 - c)

    neighbour = {("A", 1): own_index(1, 0), ("A", -1): own_index(-1, 0), ("B", 1): own_index(0, 1), ("B", -1): own_index(0, -1)}
    peers = [lax.rem(t + d, tp) for d in range(1, tp)]

    class Gather:
        def __init__(self, number, buffer, by_slot):
            self.base, self.buffer, self.by_slot = number * N_COPIES, buffer, by_slot
            self.half_rows = buffer.shape[1] // 2

        def view(self, index, half):
            if half is None:
                return self.buffer.at[index]
            return self.buffer.at[index, pl.ds(half * self.half_rows, self.half_rows)]

        def own(self, place):
            return OWN_SLOT[place] if self.by_slot else own_index(*place)

        def ring(self, i):
            axis, sign, source, half, landing = RING[i]
            at = self.own(source)
            to = OWN_SLOT[landing] if self.by_slot else at
            return pltpu.make_async_remote_copy(
                src_ref=self.view(at, half), dst_ref=self.view(to, half),
                send_sem=send_sem.at[self.base + i], recv_sem=recv_sem.at[self.base + i],
                device_id=(neighbour[axis, sign], t), device_id_type=MESH)

        def ring_arrival(self, i):
            half, landing = RING[i][3:]
            here = self.view(self.own(landing), half)
            return pltpu.make_async_remote_copy(
                src_ref=here, dst_ref=here,
                send_sem=send_sem.at[self.base + i], recv_sem=recv_sem.at[self.base + i],
                device_id=(partner, t), device_id_type=MESH)

        def push(self, place):
            i = self.base + len(RING) + PLACES.index(place)
            at = self.own(place)
            to = PARTNER_SLOT[place] if self.by_slot else at
            return pltpu.make_async_remote_copy(
                src_ref=self.view(at, None), dst_ref=self.view(to, None),
                send_sem=send_sem.at[i], recv_sem=recv_sem.at[i],
                device_id=(partner, t), device_id_type=MESH)

        def push_arrival(self, place):
            i = self.base + len(RING) + PLACES.index(place)
            here = self.view(PARTNER_SLOT[place] if self.by_slot else partner_index(*place), None)
            return pltpu.make_async_remote_copy(
                src_ref=here, dst_ref=here, send_sem=send_sem.at[i], recv_sem=recv_sem.at[i],
                device_id=(partner, t), device_id_type=MESH)

        def stage(self, number):
            waits, sends, pushes = STAGES[number - 1]
            for i in waits:
                self.ring_arrival(i).wait_recv()
            for i in sends:
                self.ring(i).start()
            for place in pushes:
                self.push(place).start()

        def from_partner(self, *places):
            for place in places:
                self.push_arrival(place).wait_recv()

        def drain(self):
            for i in range(len(RING)):
                self.ring(i).wait_send()
            for place in PLACES:
                self.push(place).wait_send()

    kvs, gus, downs = Gather(0, kv, True), Gather(1, gu, False), Gather(2, dt, False)

    rows = gate_hbm.shape[0]
    to_gate = pltpu.make_async_copy(gate_hbm, gu.at[a, pl.ds(0, rows)], local_sem.at[0])
    to_up = pltpu.make_async_copy(up_hbm, gu.at[a, pl.ds(rows, rows)], local_sem.at[1])
    to_down = pltpu.make_async_copy(down_hbm, dt.at[a], local_sem.at[2])
    to_res = pltpu.make_async_copy(res_hbm, res.at[t], local_sem.at[3])
    to_ow = pltpu.make_async_copy(ow_hbm, ow, local_sem.at[4])
    to_res.start()
    to_gate.start()
    to_up.start()
    to_down.start()
    to_ow.start()

    barrier = pltpu.get_barrier_semaphore()
    for other in [*neighbour.values(), partner]:
        pl.semaphore_signal(barrier, inc=1, device_id=(other, t), device_id_type=MESH)
    for other in peers:
        pl.semaphore_signal(barrier, inc=1, device_id=(a, other), device_id_type=MESH)

    cosine, sine = cos_ref[...], sin_ref[...]
    lane = lax.broadcasted_iota(jnp.int32, cosine.shape, 1)
    low = lax.rem(lax.div(lane, 32), 2) == 0

    def rotated(x, gain):
        x = normalized(x.astype(jnp.float32)) * gain
        swapped = jnp.where(low, pltpu.roll(x, 96, 1), pltpu.roll(x, 32, 1))
        return x * cosine + swapped * sine

    tok = k_ref.shape[0]
    kv[0, 0:tok, :] = rotated(k_ref[...], kg_ref[...]).astype(jnp.bfloat16)
    for b in range(tok // 128):
        block = v_ref[b * 128:(b + 1) * 128, :].astype(jnp.float32)
        kv[0, tok + b * 128:tok + (b + 1) * 128, :] = block.T.astype(jnp.bfloat16)

    pl.semaphore_wait(barrier, len(neighbour) + 1 + len(peers))
    kvs.stage(1)

    def x_copy(src, dst, i, other):
        return pltpu.make_async_remote_copy(src_ref=src, dst_ref=dst, send_sem=x_send.at[i], recv_sem=x_recv.at[i],
                                            device_id=(a, other), device_id_type=MESH)

    def res_copy(d):
        return x_copy(res.at[t], res.at[t], d - 1, lax.rem(t + d, tp))

    def att_copy(block, d):
        return x_copy(att.at[block, t], att.at[block, t], 3 + block * 3 + d - 1, lax.rem(t + d, tp))

    def part_copy(column, d):
        other = lax.rem(t + d, tp)
        return x_copy(part.at[column, other], recv.at[column, d - 1], 15 + column * 3 + d - 1, other)

    def x_arrival(dst, i):
        return x_copy(dst, dst, i, lax.rem(t + 1, tp))

    to_res.wait()
    for d in range(1, tp):
        res_copy(d).start()

    heads = q_ref.shape[1] // 128
    blocks = tok // 128
    for h in range(heads):
        rot = rotated(q_ref[:, h * 128:(h + 1) * 128], qg_ref[...]).astype(jnp.bfloat16)
        scaled = rot.astype(jnp.float32) * LOG2_SCALE
        for b in range(blocks):
            turned = scaled[b * 128:(b + 1) * 128, :].T
            high = turned.astype(jnp.bfloat16)
            at = (b * heads + h) * 128
            qt[0:128, at:at + 128] = high
            qt[128:256, at:at + 128] = (turned - high.astype(jnp.float32)).astype(jnp.bfloat16)

    m_ref[...] = jnp.full_like(m_ref, -1e30)
    l_ref[...] = jnp.zeros_like(l_ref)
    acc[...] = jnp.zeros_like(acc)
    buffers = [s0, s1]

    def columns(j):
        return pl.ds(pl.multiple_of(j * UNIT, UNIT), UNIT)

    def score(chunk, j, into):
        keys = kv[pl.ds(chunk * 2, 2), 0:tok, :].reshape(2 * tok, 128)
        into[...] = jnp.dot(jnp.concatenate([keys, keys], axis=1), qt[:, columns(j)], preferred_element_type=jnp.float32)

    def absorb(chunk, j, held):
        turned = jnp.concatenate(
            [kv[chunk * 2 + h, tok + b * 128:tok + (b + 1) * 128, :] for h in range(2) for b in range(blocks)], axis=1)
        at = columns(j)
        scores = held[...]
        before = m_ref[:, at]
        highest = jnp.maximum(before, jnp.max(scores, axis=0, keepdims=True))
        weights = jnp.exp2(scores - highest)
        factor = jnp.exp2(before - highest)
        m_ref[:, at] = highest
        l_ref[:, at] = l_ref[:, at] * factor + jnp.sum(weights, axis=0, keepdims=True)
        acc[:, at] = acc[:, at] * factor + jnp.dot(turned, weights.astype(jnp.bfloat16), preferred_element_type=jnp.float32)

    def weights_start():
        to_gate.wait()
        to_up.wait()
        gus.stage(1)

    def downs_start():
        to_down.wait()
        downs.stage(1)

    events = {
        0: [lambda: kvs.stage(2), weights_start],
        2: [lambda: kvs.from_partner((-1, 0), (1, 0))],
        3: [lambda: kvs.from_partner((0, -1), (0, 1))],
        4: [lambda: kvs.stage(3)],
        7: [lambda: kvs.from_partner((2, 0), (0, 2))],
        8: [lambda: kvs.from_partner((-1, -1), (-1, 1)), lambda: kvs.stage(4)],
        9: [lambda: kvs.from_partner((1, -1), (1, 1)), lambda: gus.stage(2)],
    }
    kvs.from_partner((0, 0))
    score(0, 0, s0)
    n_units = blocks * heads * 128 // UNIT

    def first_phase(k, carry):
        for j in range(n_units):
            if j + 1 < n_units:
                score(k, j + 1, buffers[(j + 1) % 2])
            else:
                for at, todo in events.items():
                    @pl.when(k == at)
                    def _():
                        for event in todo:
                            event()
                score(k + 1, 0, buffers[0])
            absorb(k, j, buffers[j % 2])
        return carry

    lax.fori_loop(0, PHASE1, first_phase, 0)

    last = kv.shape[0] // 2
    before_chunk = {
        13: [lambda: kvs.from_partner((2, -1), (2, 1))],
        14: [lambda: kvs.stage(5), lambda: kvs.from_partner((-1, 2), (1, 2))],
        15: [lambda: kvs.from_partner((2, 2))],
    }
    after_tile = {0: [downs_start], 2: [lambda: gus.stage(3)], 3: [lambda: downs.stage(2)]}

    def second_phase(j, carry):
        for k in range(PHASE1, last):
            i = k - PHASE1
            if k + 1 < last:
                if k + 1 in before_chunk:
                    @pl.when(j == 0)
                    def _():
                        for event in before_chunk[k + 1]:
                            event()
                score(k + 1, j, buffers[(i + 1) % 2])
            else:
                score(PHASE1, lax.rem(j + 1, n_units), buffers[(i + 1) % 2])
            absorb(k, j, buffers[i % 2])
        at = columns(j)
        mixed = acc[:, at] / l_ref[:, at]
        for h in range(heads):
            att[j, t, :, h * 128:(h + 1) * 128] = mixed[:, h * 128:(h + 1) * 128].T.astype(jnp.bfloat16)
        for tile, todo in after_tile.items():
            @pl.when(j == tile)
            def _():
                for event in todo:
                    event()
        for d in range(1, tp):
            att_copy(j, d).start()
        return carry

    lax.fori_loop(0, n_units, second_phase, 0)

    to_ow.wait()
    for d in range(1, tp):
        x_arrival(res.at[lax.rem(t + d, tp)], tp - d - 1).wait_recv()

    after_block = {2: [lambda: gus.stage(4)], 3: [lambda: downs.stage(3)]}

    def project(b, carry):
        for d in range(1, tp):
            x_arrival(att.at[b, lax.rem(t + d, tp)], 3 + b * 3 + tp - d - 1).wait_recv()
        rows_in = jnp.concatenate([att[b, s] for s in range(tp)], axis=1)

        def column_block(i, inner):
            at = pl.ds(pl.multiple_of(i * 256, 256), 256)
            proj[:, at] = jnp.dot(rows_in, ow[:, at], preferred_element_type=jnp.float32)
            return inner

        lax.fori_loop(0, ow.shape[1] // 256, column_block, 0)

        def row_block(i, inner):
            at = pl.ds(pl.multiple_of(i * 16, 16), 16)
            stream = (res[b, at, :].astype(jnp.float32) + og_ref[...] * normalized(proj[at, :])).astype(jnp.bfloat16)
            mid[b, at, :] = stream
            nrm[pl.ds(pl.multiple_of(b * 128 + i * 16, 16), 16), :] = (mg_ref[...] * normalized(stream.astype(jnp.float32))).astype(jnp.bfloat16)
            return inner

        lax.fori_loop(0, 8, row_block, 0)
        for block, todo in after_block.items():
            @pl.when(b == block)
            def _():
                for event in todo:
                    event()
        return carry

    lax.fori_loop(0, blocks, project, 0)

    gus.stage(5)
    gus.from_partner(*PLACES)

    def hidden_block(i, carry):
        at = pl.ds(pl.multiple_of(i * 128, 128), 128)
        width = gu.shape[0] * rows
        both = jnp.concatenate([gu[:, 0:rows, at].reshape(width, 128), gu[:, rows:2 * rows, at].reshape(width, 128)], axis=1)
        gated = jnp.dot(nrm[...], both, preferred_element_type=jnp.float32)
        gate, up = gated[:, 0:128], gated[:, 128:256]
        hid[:, at] = (gate / (1.0 + jnp.exp(-gate)) * up).astype(jnp.bfloat16)
        return carry

    lax.fori_loop(0, gu.shape[2] // 128, hidden_block, 0)

    downs.stage(4)
    downs.stage(5)
    downs.from_partner(*PLACES)
    per_block = 256 // rows
    n_columns = dt.shape[0] // per_block

    def down_block(i, carry):
        weight = dt[pl.ds(i * per_block, per_block)].reshape(256, dt.shape[2])
        share = lax.dot_general(hid[...], weight, (((1,), (1,)), ((), ())), preferred_element_type=jnp.float32).astype(jnp.bfloat16)
        for b in range(blocks):
            part[i, b] = share[b * 128:(b + 1) * 128, :]

        @pl.when(i > 0)
        def _():
            for d in range(1, tp):
                part_copy(i - 1, d).start()
        return carry

    lax.fori_loop(0, n_columns, down_block, 0)
    for d in range(1, tp):
        part_copy(n_columns - 1, d).start()

    def arrived(i, carry):
        for d in range(1, tp):
            x_arrival(recv.at[i, d - 1], 15 + i * 3 + d - 1).wait_recv()
        return carry

    lax.fori_loop(0, n_columns, arrived, 0)

    def finish(i, carry):
        at = pl.ds(pl.multiple_of(i * 16, 16), 16)
        total = []
        for k in range(n_columns):
            one = part[k, t, at, :].astype(jnp.float32)
            for d in range(tp - 1):
                one = one + recv[k, d, at, :].astype(jnp.float32)
            total.append(one)
        branch = jnp.concatenate(total, axis=1)
        out_ref[at, :] = (mid[t, at, :].astype(jnp.float32) + fg_ref[...] * normalized(branch)).astype(jnp.bfloat16)
        return carry

    lax.fori_loop(0, 8, finish, 0)

    for gather in (kvs, gus, downs):
        gather.drain()
    for d in range(1, tp):
        res_copy(d).wait_send()
        for b in range(blocks):
            att_copy(b, d).wait_send()

    def drained(i, carry):
        for d in range(1, tp):
            part_copy(i, d).wait_send()
        return carry

    lax.fori_loop(0, n_columns, drained, 0)


def on_device(queries, keys, values, q_gain, k_gain, out_weight, out_gain, residual_in, mlp_gain, gate_weight, up_weight, down_weight, final_gain):
    sp, tp = lax.axis_size("sp"), lax.axis_size("tp")
    n = math.isqrt(sp // 2)
    tok, head = keys.shape
    rows, hidden = gate_weight.shape
    width = out_weight.shape[1]
    quarter = head // 4
    freqs = 10000.0 ** (-jnp.arange(quarter, dtype=jnp.float32) / quarter)
    grid_rows = tok // GRID_W
    row_angle = (lax.axis_index("sp") * grid_rows + jnp.arange(grid_rows, dtype=jnp.int32)).astype(jnp.float32)[:, None] * freqs
    column_angle = jnp.arange(GRID_W, dtype=jnp.int32).astype(jnp.float32)[:, None] * freqs
    shape = (grid_rows, GRID_W, quarter)

    def table(function, signs):
        by_row = jnp.broadcast_to(function(row_angle)[:, None], shape)
        by_column = jnp.broadcast_to(function(column_angle)[None], shape)
        return jnp.concatenate([signs[0] * by_row, signs[1] * by_row, signs[0] * by_column, signs[1] * by_column], axis=-1).reshape(tok, head)

    blocks = tok // 128
    bf16, f32 = jnp.bfloat16, jnp.float32
    vmem = pl.BlockSpec(memory_space=pltpu.VMEM)
    anywhere = pl.BlockSpec(memory_space=pl.ANY)
    n_columns = width // 256
    q_columns = tok * queries.shape[1] // head
    return pl.pallas_call(
        functools.partial(layer_kernel, n, tp),
        out_shape=jax.ShapeDtypeStruct(residual_in.shape, bf16),
        in_specs=[vmem] * 10 + [anywhere] * 5,
        out_specs=vmem,
        scratch_shapes=[
            pltpu.VMEM((sp, 2 * tok, head), bf16),
            pltpu.VMEM((sp, 2 * rows, hidden), bf16),
            pltpu.VMEM((sp, rows, hidden), bf16),
            pltpu.VMEM(out_weight.shape, bf16),
            pltpu.VMEM((tp, *residual_in.shape), bf16),
            pltpu.VMEM((blocks, tp, 128, queries.shape[1]), bf16),
            pltpu.VMEM((blocks, 128, width), bf16),
            pltpu.VMEM((tok, width), bf16),
            pltpu.VMEM((tok, hidden), bf16),
            pltpu.VMEM((n_columns, blocks, 128, 256), bf16),
            pltpu.VMEM((n_columns, tp - 1, 128, 256), bf16),
            pltpu.VMEM((128, width), f32),
            pltpu.VMEM((2 * head, q_columns), bf16),
            pltpu.VMEM((2 * tok, UNIT), f32),
            pltpu.VMEM((2 * tok, UNIT), f32),
            pltpu.VMEM((head, q_columns), f32),
            pltpu.VMEM((1, q_columns), f32),
            pltpu.VMEM((1, q_columns), f32),
            pltpu.SemaphoreType.DMA((3 * N_COPIES,)),
            pltpu.SemaphoreType.DMA((3 * N_COPIES,)),
            pltpu.SemaphoreType.DMA((39,)),
            pltpu.SemaphoreType.DMA((39,)),
            pltpu.SemaphoreType.DMA((5,)),
        ],
        compiler_params=pltpu.CompilerParams(collective_id=0, has_side_effects=True, vmem_limit_bytes=67043328),
        name="layer",
    )(queries, keys, values, table(jnp.cos, (1.0, 1.0)), table(jnp.sin, (-1.0, 1.0)),
      q_gain[None], k_gain[None], out_gain[None], mlp_gain[None], final_gain[None],
      out_weight, residual_in, gate_weight, up_weight, down_weight.T)


def solution(mesh):
    return jax.shard_map(
        on_device,
        mesh=mesh,
        in_specs=(
            P("sp", "tp"), P("sp", "tp"), P("sp", "tp"), P(), P(), P(), P(), P(("sp", "tp"), None), P(),
            P("sp", "tp"), P("sp", "tp"), P("tp", "sp"), P(),
        ),
        out_specs=P(("sp", "tp"), None),
        check_vma=False,
    )
```

```python
import functools
import math

import jax
import jax.numpy as jnp
import numpy as np
from jax import lax
from jax.experimental import pallas as pl
from jax.experimental.pallas import tpu as pltpu
from jax.sharding import PartitionSpec as P

GRID_W = 64
MESH = pl.DeviceIdType.MESH
EPS = 1e-06
LOG2_SCALE = 128 ** (-0.5) * math.log2(math.e)
UNIT = 512
PHASE1 = 8

RING = [
    ("A", 1, (0, 0), None, (-1, 0)),
    ("A", -1, (0, 0), None, (1, 0)),
    ("B", 1, (0, 0), None, (0, -1)),
    ("B", -1, (0, 0), None, (0, 1)),
    ("A", 1, (-1, 0), 0, (2, 0)),
    ("A", -1, (1, 0), 1, (2, 0)),
    ("B", 1, (-1, 0), None, (-1, -1)),
    ("B", -1, (-1, 0), None, (-1, 1)),
    ("B", 1, (1, 0), None, (1, -1)),
    ("B", -1, (1, 0), None, (1, 1)),
    ("B", 1, (0, -1), 0, (0, 2)),
    ("B", -1, (0, 1), 1, (0, 2)),
    ("B", 1, (2, 0), None, (2, -1)),
    ("B", -1, (2, 0), None, (2, 1)),
    ("B", 1, (-1, -1), 0, (-1, 2)),
    ("B", -1, (-1, 1), 1, (-1, 2)),
    ("B", 1, (1, -1), 0, (1, 2)),
    ("B", -1, (1, 1), 1, (1, 2)),
    ("B", 1, (2, -1), 0, (2, 2)),
    ("B", -1, (2, 1), 1, (2, 2)),
]
PLACES = [(0, 0), (-1, 0), (1, 0), (0, -1), (0, 1), (2, 0), (0, 2), (-1, -1), (-1, 1), (1, -1), (1, 1), (2, -1), (2, 1), (-1, 2), (1, 2), (2, 2)]
STAGES = {
    "1A": (None, [0, 1], [(0, 0)]),
    "1B": (None, [2, 3], []),
    "2A": (0, [4, 5, 6, 7, 8, 9], [(-1, 0), (1, 0)]),
    "2B": (1, [10, 11], [(0, -1), (0, 1)]),
    "3": (2, [12, 13, 14, 15, 16, 17], [(2, 0), (0, 2), (-1, -1), (-1, 1), (1, -1), (1, 1)]),
    "4": (3, [18, 19], [(2, -1), (2, 1), (-1, 2), (1, 2)]),
    "5": (4, [], [(2, 2)]),
}
RING_GROUPS = [[0, 1], [2, 3], [4, 5, 6, 7, 8, 9, 10, 11], [12, 13, 14, 15, 16, 17], [18, 19]]
OWN_SLOT = {(0, 0): 0, (-1, 0): 2, (1, 0): 3, (0, -1): 6, (0, 1): 7, (2, 0): 10, (0, 2): 11, (-1, -1): 12, (-1, 1): 13, (1, -1): 14, (1, 1): 15,
            (2, -1): 22, (2, 1): 23, (-1, 2): 24, (1, 2): 25, (2, 2): 30}
PARTNER_SLOT = {(0, 0): 1, (-1, 0): 4, (1, 0): 5, (0, -1): 8, (0, 1): 9, (2, 0): 16, (0, 2): 17, (-1, -1): 18, (-1, 1): 19, (1, -1): 20, (1, 1): 21,
                (2, -1): 26, (2, 1): 27, (-1, 2): 28, (1, 2): 29, (2, 2): 31}
RING_GROUP = {i: number for number, group in enumerate(RING_GROUPS) for i in group}
RING_SHARDS = [sum(2 if RING[i][3] is None else 1 for i in group) // 2 for group in RING_GROUPS]
PUSH_GROUPS = [PLACES[0:1], PLACES[1:3], PLACES[3:5], PLACES[5:7], PLACES[7:9], PLACES[9:11], PLACES[11:13], PLACES[13:15], PLACES[15:16]]
PUSH_GROUP = {place: number for number, group in enumerate(PUSH_GROUPS) for place in group}
N_GROUPS = len(RING_SHARDS) + len(PUSH_GROUPS)
ALL_SHARDS = sum(RING_SHARDS) + len(PLACES)


def normalized(x):
    return x * lax.rsqrt(jnp.mean(x * x, axis=-1, keepdims=True) + EPS)


def layer_kernel(n, tp, q_ref, k_ref, v_ref, cos_row, cos_col, sin_row, sin_col, qg_ref, kg_ref, og_ref, mg_ref, fg_ref,
                 ow_hbm, res_hbm, gate_hbm, up_hbm, down_hbm, out_ref,
                 keys, vals, gates, ups, dt, ow, res, att, mid, nrm, hid, part, recv, proj, proj_b, qt, s0, s1, acc, m_ref, l_ref,
                 send_sem, recv_sem, x_send, x_recv, local_sem):
    a = lax.axis_index("sp")
    t = lax.axis_index("tp")
    c = lax.rem(a, 2)
    chip = lax.div(a, 2)
    z = lax.div(chip, n)
    y = lax.rem(chip, n)
    u = y * (1 - c) + z * c
    w = z * (1 - c) + y * c
    partner = a + 1 - 2 * c

    def device_at(uu, ww, cc):
        return ((ww * (1 - cc) + uu * cc) * n + uu * (1 - cc) + ww * cc) * 2 + cc

    def own_index(du, dw):
        return device_at(lax.rem(u + du + n, n), lax.rem(w + dw + n, n), c)

    def partner_index(du, dw):
        return device_at(lax.rem(w + du + n, n), lax.rem(u + dw + n, n), 1 - c)

    neighbour = {("A", 1): own_index(1, 0), ("A", -1): own_index(-1, 0), ("B", 1): own_index(0, 1), ("B", -1): own_index(0, -1)}
    peers = [lax.rem(t + d, tp) for d in range(1, tp)]

    class Gather:
        def __init__(self, number, buffer, own, given, kept):
            self.number, self.buffer, self.own, self.given, self.kept = number, buffer, own, given, kept
            self.half_rows = buffer.shape[1] // 2

        def view(self, index, half=None):
            if half is None:
                return self.buffer.at[index]
            return self.buffer.at[index, pl.ds(half * self.half_rows, self.half_rows)]

        def copy(self, src, dst, group, target):
            return pltpu.make_async_remote_copy(
                src_ref=src, dst_ref=dst, send_sem=send_sem.at[self.number], recv_sem=recv_sem.at[self.number * N_GROUPS + group],
                device_id=(target, t), device_id_type=MESH)

        def ring(self, i):
            axis, sign, source, half, landing = RING[i]
            at = self.own(source)
            to = at if self.own is own_index_of else self.own(landing)
            return self.copy(self.view(at, half), self.view(to, half), RING_GROUP[i], neighbour[axis, sign])

        def push(self, place):
            return self.copy(self.view(self.own(place)), self.view(self.given(place)), len(RING_SHARDS) + PUSH_GROUP[place], partner)

        def shards(self, count, group):
            these = self.buffer.at[pl.ds(0, count)]
            return self.copy(these, these, group, partner)

        def stage(self, name):
            group, sends, places = STAGES[name]
            if group is not None:
                self.shards(RING_SHARDS[group], group).wait_recv()
            for i in sends:
                self.ring(i).start()
            for place in places:
                self.push(place).start()

        def from_partner(self, *groups):
            for group in groups:
                self.shards(len(PUSH_GROUPS[group]), len(RING_SHARDS) + group).wait_recv()

        def drain(self):
            self.shards(ALL_SHARDS, 0).wait_send()

    def own_index_of(place):
        return own_index(*place)

    def chip_slot(place, core):
        return PLACES.index(place) * 2 + core

    by_slot = (OWN_SLOT.get, PARTNER_SLOT.get, PARTNER_SLOT.get)
    by_index = (own_index_of, own_index_of, lambda place: partner_index(*place))
    ks, vs = Gather(0, keys, *by_slot), Gather(1, vals, *by_slot)
    gs, us = Gather(2, gates, *by_index), Gather(3, ups, *by_index)
    downs = Gather(4, dt, lambda place: chip_slot(place, c), lambda place: chip_slot(place[::-1], c),
                   lambda place: chip_slot(place[::-1], 1 - c))

    rows = gate_hbm.shape[0]
    to_gate = pltpu.make_async_copy(gate_hbm, gates.at[a], local_sem.at[0])
    to_up = pltpu.make_async_copy(up_hbm, ups.at[a], local_sem.at[1])
    to_down = pltpu.make_async_copy(down_hbm, dt.at[chip_slot((0, 0), c)], local_sem.at[2])
    to_res = pltpu.make_async_copy(res_hbm, res.at[t], local_sem.at[3])
    to_ow = pltpu.make_async_copy(ow_hbm, ow, local_sem.at[4])
    to_res.start()
    to_gate.start()
    to_up.start()
    to_down.start()
    to_ow.start()

    barrier = pltpu.get_barrier_semaphore()
    for other in [*neighbour.values(), partner]:
        pl.semaphore_signal(barrier, inc=1, device_id=(other, t), device_id_type=MESH)
    for other in peers:
        pl.semaphore_signal(barrier, inc=1, device_id=(a, other), device_id_type=MESH)

    tok = k_ref.shape[0]
    grid_rows = tok // GRID_W

    def table(by_row, by_column):
        mine = by_row[pl.ds(a * grid_rows, grid_rows), :]
        return jnp.concatenate([mine[r:r + 1] + by_column[...] for r in range(grid_rows)], axis=0)

    cosine, sine = table(cos_row, cos_col), table(sin_row, sin_col)
    lane = lax.broadcasted_iota(jnp.int32, cosine.shape, 1)
    low = lax.rem(lax.div(lane, 32), 2) == 0

    def rotated(x, gain):
        x = normalized(x.astype(jnp.float32)) * gain
        swapped = jnp.where(low, pltpu.roll(x, 96, 1), pltpu.roll(x, 32, 1))
        return x * cosine + swapped * sine

    keys[0] = rotated(k_ref[...], kg_ref[...]).astype(jnp.bfloat16)
    for b in range(tok // 128):
        block = v_ref[b * 128:(b + 1) * 128, :].astype(jnp.float32)
        vals[0, b * 128:(b + 1) * 128, :] = block.T.astype(jnp.bfloat16)

    heads = q_ref.shape[1] // 128
    blocks = tok // 128
    part_rows = 128 // tp
    for h in range(heads):
        rot = rotated(q_ref[:, h * 128:(h + 1) * 128], qg_ref[...]).astype(jnp.bfloat16)
        scaled = rot.astype(jnp.float32) * LOG2_SCALE
        for b in range(blocks):
            turned = jnp.concatenate([scaled[o * 128 + b * part_rows:o * 128 + (b + 1) * part_rows] for o in range(tp)], axis=0).T
            high = turned.astype(jnp.bfloat16)
            at = (b * heads + h) * 128
            qt[0:128, at:at + 128] = high
            qt[128:256, at:at + 128] = (turned - high.astype(jnp.float32)).astype(jnp.bfloat16)

    m_ref[...] = jnp.full_like(m_ref, -1e30)
    l_ref[...] = jnp.zeros_like(l_ref)
    acc[...] = jnp.zeros_like(acc)

    pl.semaphore_wait(barrier, len(neighbour) + 1 + len(peers))
    ks.stage("1A")
    vs.stage("1A")

    def x_copy(src, dst, kind, group, other):
        return pltpu.make_async_remote_copy(src_ref=src, dst_ref=dst, send_sem=x_send.at[kind], recv_sem=x_recv.at[group],
                                            device_id=(a, other), device_id_type=MESH)

    def res_copy(d):
        return x_copy(res.at[t], res.at[t], 0, 0, lax.rem(t + d, tp))

    def att_copy(block, d):
        return x_copy(att.at[block, t], att.at[block, t], 1, 1 + block, lax.rem(t + d, tp))

    def part_copy(half, column, d):
        other = lax.rem(t + d, tp)
        return x_copy(part.at[half, column, other], recv.at[half, column, d - 1], 2 + half, 5 + half * part.shape[1] + column, other)

    def x_all(these, kind, group):
        return x_copy(these, these, kind, group, lax.rem(t + 1, tp))

    to_res.wait()
    for d in range(1, tp):
        res_copy(d).start()

    buffers = [s0, s1]

    def columns(j):
        return pl.ds(pl.multiple_of(j * UNIT, UNIT), UNIT)

    def score(chunk, j, into):
        rows_in = keys[pl.ds(chunk * 2, 2)].reshape(2 * tok, 128)
        into[...] = jnp.dot(jnp.concatenate([rows_in, rows_in], axis=1), qt[:, columns(j)], preferred_element_type=jnp.float32)

    def absorb(chunk, j, held):
        turned = jnp.concatenate(
            [vals[chunk * 2 + h, b * 128:(b + 1) * 128, :] for h in range(2) for b in range(blocks)], axis=1)
        at = columns(j)
        scores = held[...]
        before = m_ref[:, at]
        highest = jnp.maximum(before, jnp.max(scores, axis=0, keepdims=True))
        weights = jnp.exp2(scores - highest)
        factor = jnp.exp2(before - highest)
        m_ref[:, at] = highest
        l_ref[:, at] = l_ref[:, at] * factor + jnp.sum(weights, axis=0, keepdims=True)
        acc[:, at] = acc[:, at] * factor + jnp.dot(turned, weights.astype(jnp.bfloat16), preferred_element_type=jnp.float32)

    def both(*groups):
        for gather in (ks, vs):
            gather.from_partner(*groups)

    events = {
        (0, 2): [lambda: ks.stage("1B"), lambda: vs.stage("1B"), lambda: to_down.wait(), lambda: downs.stage("1A"), lambda: ks.stage("2A")],
        (1, 0): [lambda: vs.stage("2A")],
        (1, 2): [lambda: ks.stage("2B"), lambda: both(1)],
        (2, 2): [lambda: vs.stage("2B")],
        (3, 2): [lambda: both(2)],
        (4, 0): [lambda: ks.stage("3")],
        (4, 2): [lambda: vs.stage("3"), lambda: to_gate.wait(), lambda: gs.stage("1A"), lambda: gs.stage("1B")],
        (6, 2): [lambda: ks.stage("4")],
        (7, 2): [lambda: both(3), lambda: vs.stage("4"), lambda: to_up.wait(), lambda: us.stage("1A"), lambda: us.stage("1B")],
    }
    ks.from_partner(0)
    score(0, 0, s0)
    vs.from_partner(0)
    n_units = blocks * heads * 128 // UNIT

    def run(table, index, *unit):
        for at, todo in table.items():
            if at[1:] == unit:
                @pl.when(index == at[0])
                def _():
                    for event in todo:
                        event()

    def first_phase(k, carry):
        for j in range(n_units):
            if j % 2 == 0:
                run(events, k, j)
            if j + 1 < n_units:
                score(k, j + 1, buffers[(j + 1) % 2])
            else:
                score(k + 1, 0, buffers[0])
            absorb(k, j, buffers[j % 2])
        return carry

    lax.fori_loop(0, PHASE1, first_phase, 0)

    last = keys.shape[0] // 2
    later = {
        (0, 8): [lambda: both(4, 5)],
        (0, 12): [lambda: both(6, 7), lambda: gs.stage("2A"), lambda: gs.stage("2B")],
        (0, 14): [lambda: ks.stage("5"), lambda: vs.stage("5"), lambda: both(8)],
        (1, 12): [lambda: us.stage("2A"), lambda: us.stage("2B")],
        (2, 12): [lambda: gs.stage("3")],
        (3, 12): [lambda: us.stage("3"), lambda: downs.stage("1B")],
    }

    def second_phase(j, carry):
        for k in range(PHASE1, last):
            i = k - PHASE1
            if i % 2 == 0:
                run(later, j, k)
            if k + 1 < last:
                score(k + 1, j, buffers[(i + 1) % 2])
            else:
                score(PHASE1, lax.rem(j + 1, n_units), buffers[(i + 1) % 2])
            absorb(k, j, buffers[i % 2])
        at = columns(j)
        mixed = acc[:, at] / l_ref[:, at]
        for h in range(heads):
            att[j, t, :, h * 128:(h + 1) * 128] = mixed[:, h * 128:(h + 1) * 128].T.astype(jnp.bfloat16)
        for d in range(1, tp):
            att_copy(j, d).start()
        return carry

    lax.fori_loop(0, n_units, second_phase, 0)

    to_ow.wait()
    x_all(res.at[pl.ds(0, tp - 1)], 0, 0).wait_recv()


    quarters = 4
    width_part = ow.shape[1] // quarters

    def dots(b, into, i):
        rows_in = jnp.concatenate([att[b, s] for s in range(tp)], axis=1)
        at = slice(i * width_part, (i + 1) * width_part)
        into[:, at] = jnp.dot(rows_in, ow[:, at], preferred_element_type=jnp.float32)

    def norms(b, held, i):
        mine = slice(b * part_rows, (b + 1) * part_rows)
        at = slice(i * part_rows, (i + 1) * part_rows)
        stream = (res[i, mine, :].astype(jnp.float32) + og_ref[...] * normalized(held[at, :])).astype(jnp.bfloat16)
        mid[i, mine, :] = stream
        nrm[b * 128 + i * part_rows:b * 128 + (i + 1) * part_rows, :] = (
            mg_ref[...] * normalized(stream.astype(jnp.float32))).astype(jnp.bfloat16)

    half_rows = tok // 2

    projected = [proj, proj_b]

    def project(first, count, after):
        for b in range(first, first + count + 1):
            now = b < first + count
            if now:
                x_all(att.at[b, pl.ds(0, tp - 1)], 1, 1 + b).wait_recv()
            for i in range(quarters):
                if now:
                    dots(b, projected[b % 2], i)
                if b > first:
                    norms(b - 1, projected[(b - 1) % 2], i)
            for event in after.get((b,), []):
                event()

    width = gates.shape[0] * rows
    n_hidden = gates.shape[2] // 128

    def feed(half, first, last_one):
        these = slice(half * half_rows, (half + 1) * half_rows)

        def gated_dot(i, into):
            at = pl.ds(pl.multiple_of(i * 128, 128), 128)
            pair = jnp.concatenate([gates[:, :, at].reshape(width, 128), ups[:, :, at].reshape(width, 128)], axis=1)
            into[0:half_rows, 0:256] = jnp.dot(nrm[these, :], pair, preferred_element_type=jnp.float32)

        def gating(i, held):
            gate, up = held[0:half_rows, 0:128], held[0:half_rows, 128:256]
            hid[these, pl.ds(pl.multiple_of(i * 128, 128), 128)] = (gate / (1.0 + jnp.exp(-gate)) * up).astype(jnp.bfloat16)

        gated_dot(first, s0)
        pairs = (last_one - first - 1) // 2

        def hidden_pair(i, carry):
            at = first + 2 * i
            gated_dot(at + 1, s1)
            gating(at, s0)
            gated_dot(at + 2, s0)
            gating(at + 1, s1)
            return carry

        lax.fori_loop(0, pairs, hidden_pair, 0)
        at = first + 2 * pairs
        if at + 1 < last_one:
            gated_dot(at + 1, s1)
            gating(at, s0)
            gating(at + 1, s1)
        else:
            gating(at, s0)

    per_block = 256 // rows
    n_columns = dt.shape[0] // per_block
    owned = half_rows // tp

    def shrink(half, first, count, before):
        these = slice(half * half_rows, (half + 1) * half_rows)

        def down_block(i, carry):
            run(before, i)
            weight = dt[pl.ds(i * per_block, per_block)].reshape(256, dt.shape[2])
            share = lax.dot_general(hid[these, :], weight, (((1,), (1,)), ((), ())), preferred_element_type=jnp.float32).astype(jnp.bfloat16)
            for o in range(tp):
                part[half, i, o] = jnp.concatenate(
                    [share[b * 128 + o * part_rows:b * 128 + (o + 1) * part_rows] for b in range(blocks // 2)], axis=0)

            @pl.when(i > first)
            def _():
                for d in range(1, tp):
                    part_copy(half, i - 1, d).start()
            return carry

        lax.fori_loop(first, first + count, down_block, 0)
        for d in range(1, tp):
            part_copy(half, first + count - 1, d).start()

    project(0, blocks - 1, {(1,): [lambda: gs.stage("4"), lambda: us.stage("4"), lambda: downs.stage("2A")],
                            (2,): [lambda: downs.stage("2B"), lambda: gs.stage("5")]})
    us.stage("5")
    for gather in (gs, us):
        gather.from_partner(*range(len(PUSH_GROUPS)))
    feed(0, 0, n_hidden)
    downs.stage("3")
    shrink(0, 0, 5, {(0,): [lambda: downs.from_partner(0, 1, 2)], (2,): [lambda: downs.from_partner(3, 4, 5)]})
    project(blocks - 1, 1, {})
    feed(1, 0, n_hidden // 2)
    downs.stage("4")
    downs.from_partner(6, 7)
    shrink(0, 5, 2, {})
    feed(1, n_hidden // 2, n_hidden)
    downs.stage("5")
    shrink(1, 0, 7, {})
    downs.from_partner(8)
    shrink(0, 7, 1, {})
    shrink(1, 7, 1, {})

    for half, columns_of in ((0, range(7)), (1, range(7)), (0, [7]), (1, [7])):
        for i in columns_of:
            x_all(recv.at[half, i], 2, 5 + half * n_columns + i).wait_recv()
            total = part[half, i, t].astype(jnp.float32)
            for d in range(tp - 1):
                total = total + recv[half, i, d].astype(jnp.float32)
            for h in range(2):
                chip_at = lax.div(own_index(*PLACES[2 * i + h]), 2)
                proj[half * owned:(half + 1) * owned, pl.ds(pl.multiple_of(chip_at * 128, 128), 128)] = total[:, h * 128:(h + 1) * 128]

    def finish(i, carry):
        at = pl.ds(pl.multiple_of(i * 32, 32), 32)
        out_ref[at, :] = (mid[t, at, :].astype(jnp.float32) + fg_ref[...] * normalized(proj[at, :])).astype(jnp.bfloat16)
        return carry

    lax.fori_loop(0, 4, finish, 0)

    for gather in (ks, vs, gs, us, downs):
        gather.drain()
    x_all(res.at[pl.ds(0, tp - 1)], 0, 0).wait_send()
    x_all(att.at[pl.ds(0, tp - 1)], 1, 0).wait_send()
    for half in range(2):
        x_all(part.at[half, pl.ds(0, n_columns * (tp - 1) // tp)], 2 + half, 0).wait_send()


def on_device(queries, keys, values, q_gain, k_gain, out_weight, out_gain, residual_in, mlp_gain, gate_weight, up_weight, down_weight, final_gain):
    sp, tp = lax.axis_size("sp"), lax.axis_size("tp")
    n = math.isqrt(sp // 2)
    tok, head = keys.shape
    rows, hidden = gate_weight.shape
    width = out_weight.shape[1]
    quarter = head // 4
    freqs = np.float32(10000.0) ** (-np.arange(quarter, dtype=np.float32) / np.float32(quarter))

    def table(function, signs, count, low):
        angle = np.arange(count, dtype=np.float32)[:, None] * freqs
        values, empty = function(angle.astype(np.float64)).astype(np.float32), np.zeros((count, 2 * quarter), np.float32)
        turned = np.concatenate([signs[0] * values, signs[1] * values], axis=1)
        return jnp.asarray(np.concatenate([turned, empty] if low else [empty, turned], axis=1).astype(np.float32))

    tables = [table(function, signs, count, low) for function, signs in ((np.cos, (1.0, 1.0)), (np.sin, (-1.0, 1.0)))
              for count, low in ((sp * tok // GRID_W, True), (GRID_W, False))]
    blocks = tok // 128
    bf16, f32 = jnp.bfloat16, jnp.float32
    vmem = pl.BlockSpec(memory_space=pltpu.VMEM)
    anywhere = pl.BlockSpec(memory_space=pl.ANY)
    n_columns = width // 256
    q_columns = tok * queries.shape[1] // head
    return pl.pallas_call(
        functools.partial(layer_kernel, n, tp),
        out_shape=jax.ShapeDtypeStruct(residual_in.shape, bf16),
        in_specs=[vmem] * 12 + [anywhere] * 5,
        out_specs=vmem,
        scratch_shapes=[
            pltpu.VMEM((sp, tok, head), bf16),
            pltpu.VMEM((sp, tok, head), bf16),
            pltpu.VMEM((sp, rows, hidden), bf16),
            pltpu.VMEM((sp, rows, hidden), bf16),
            pltpu.VMEM((sp, rows, hidden), bf16),
            pltpu.VMEM(out_weight.shape, bf16),
            pltpu.VMEM((tp, *residual_in.shape), bf16),
            pltpu.VMEM((blocks, tp, 128, queries.shape[1]), bf16),
            pltpu.VMEM((blocks, 128, width), bf16),
            pltpu.VMEM((tok, width), bf16),
            pltpu.VMEM((tok, hidden), bf16),
            pltpu.VMEM((2, n_columns, tp, 64, 256), bf16),
            pltpu.VMEM((2, n_columns, tp - 1, 64, 256), bf16),
            pltpu.VMEM((128, width), f32),
            pltpu.VMEM((128, width), f32),
            pltpu.VMEM((2 * head, q_columns), bf16),
            pltpu.VMEM((2 * tok, UNIT), f32),
            pltpu.VMEM((2 * tok, UNIT), f32),
            pltpu.VMEM((head, q_columns), f32),
            pltpu.VMEM((1, q_columns), f32),
            pltpu.VMEM((1, q_columns), f32),
            pltpu.SemaphoreType.DMA((5,)),
            pltpu.SemaphoreType.DMA((5 * N_GROUPS,)),
            pltpu.SemaphoreType.DMA((4,)),
            pltpu.SemaphoreType.DMA((5 + 2 * n_columns,)),
            pltpu.SemaphoreType.DMA((5,)),
        ],
        compiler_params=pltpu.CompilerParams(collective_id=0, has_side_effects=True, vmem_limit_bytes=67043328),
        name="layer",
    )(queries, keys, values, *tables,
      q_gain[None], k_gain[None], out_gain[None], mlp_gain[None], final_gain[None],
      out_weight, residual_in, gate_weight, up_weight, down_weight.T)


def solution(mesh):
    return jax.shard_map(
        on_device,
        mesh=mesh,
        in_specs=(
            P("sp", "tp"), P("sp", "tp"), P("sp", "tp"), P(), P(), P(), P(), P(("sp", "tp"), None), P(),
            P("sp", "tp"), P("sp", "tp"), P("tp", "sp"), P(),
        ),
        out_specs=P(("sp", "tp"), None),
        check_vma=False,
    )
```

```python
import functools
import math

import jax
import jax.numpy as jnp
import numpy as np
from jax import lax
from jax.experimental import pallas as pl
from jax.experimental.pallas import tpu as pltpu
from jax.sharding import PartitionSpec as P

GRID_W = 64
MESH = pl.DeviceIdType.MESH
EPS = 1e-06
LOG2_SCALE = 128 ** (-0.5) * math.log2(math.e)
UNIT = 512
PHASE1 = 8

RING = [
    ("A", 1, (0, 0), None, (-1, 0)),
    ("A", -1, (0, 0), None, (1, 0)),
    ("B", 1, (0, 0), None, (0, -1)),
    ("B", -1, (0, 0), None, (0, 1)),
    ("A", 1, (-1, 0), 0, (2, 0)),
    ("A", -1, (1, 0), 1, (2, 0)),
    ("B", 1, (-1, 0), None, (-1, -1)),
    ("B", -1, (-1, 0), None, (-1, 1)),
    ("B", 1, (1, 0), None, (1, -1)),
    ("B", -1, (1, 0), None, (1, 1)),
    ("B", 1, (0, -1), 0, (0, 2)),
    ("B", -1, (0, 1), 1, (0, 2)),
    ("B", 1, (2, 0), None, (2, -1)),
    ("B", -1, (2, 0), None, (2, 1)),
    ("B", 1, (-1, -1), 0, (-1, 2)),
    ("B", -1, (-1, 1), 1, (-1, 2)),
    ("B", 1, (1, -1), 0, (1, 2)),
    ("B", -1, (1, 1), 1, (1, 2)),
    ("B", 1, (2, -1), 0, (2, 2)),
    ("B", -1, (2, 1), 1, (2, 2)),
]
PLACES = [(0, 0), (-1, 0), (1, 0), (0, -1), (0, 1), (2, 0), (0, 2), (-1, -1), (-1, 1), (1, -1), (1, 1), (2, -1), (2, 1), (-1, 2), (1, 2), (2, 2)]
STAGES = {
    "1A": (None, [0, 1], [(0, 0)]),
    "1B": (None, [2, 3], []),
    "2A": (0, [4, 5, 6, 7, 8, 9], [(-1, 0), (1, 0)]),
    "2B": (1, [10, 11], [(0, -1), (0, 1)]),
    "3": (2, [12, 13, 14, 15, 16, 17], [(2, 0), (0, 2), (-1, -1), (-1, 1), (1, -1), (1, 1)]),
    "4": (3, [18, 19], [(2, -1), (2, 1), (-1, 2), (1, 2)]),
    "5": (4, [], [(2, 2)]),
}
RING_GROUPS = [[0, 1], [2, 3], [4, 5, 6, 7, 8, 9, 10, 11], [12, 13, 14, 15, 16, 17], [18, 19]]
OWN_SLOT = {(0, 0): 0, (-1, 0): 2, (1, 0): 3, (0, -1): 6, (0, 1): 7, (2, 0): 10, (0, 2): 11, (-1, -1): 12, (-1, 1): 13, (1, -1): 14, (1, 1): 15,
            (2, -1): 22, (2, 1): 23, (-1, 2): 24, (1, 2): 25, (2, 2): 30}
PARTNER_SLOT = {(0, 0): 1, (-1, 0): 4, (1, 0): 5, (0, -1): 8, (0, 1): 9, (2, 0): 16, (0, 2): 17, (-1, -1): 18, (-1, 1): 19, (1, -1): 20, (1, 1): 21,
                (2, -1): 26, (2, 1): 27, (-1, 2): 28, (1, 2): 29, (2, 2): 31}
RING_GROUP = {i: number for number, group in enumerate(RING_GROUPS) for i in group}
RING_SHARDS = [sum(2 if RING[i][3] is None else 1 for i in group) // 2 for group in RING_GROUPS]
PUSH_GROUPS = [PLACES[0:1], PLACES[1:3], PLACES[3:5], PLACES[5:7], PLACES[7:9], PLACES[9:11], PLACES[11:13], PLACES[13:15], PLACES[15:16]]
PUSH_GROUP = {place: number for number, group in enumerate(PUSH_GROUPS) for place in group}
N_GROUPS = len(RING_SHARDS) + len(PUSH_GROUPS)
ALL_SHARDS = sum(RING_SHARDS) + len(PLACES)


def normalized(x):
    return x * lax.rsqrt(jnp.mean(x * x, axis=-1, keepdims=True) + EPS)


def layer_kernel(n, tp, q_ref, k_ref, v_ref, cos_row, cos_col, sin_row, sin_col, qg_ref, kg_ref, og_ref, mg_ref, fg_ref,
                 ow_hbm, res_hbm, gate_hbm, up_hbm, down_hbm, out_ref,
                 keys, vals, gates, ups, dt, ow, res, att, mid, nrm, hid, part, recv, proj, proj_b, qt, s0, s1, acc, m_ref, l_ref,
                 send_sem, recv_sem, x_send, x_recv, local_sem):
    a = lax.axis_index("sp")
    t = lax.axis_index("tp")
    c = lax.rem(a, 2)
    chip = lax.div(a, 2)
    z = lax.div(chip, n)
    y = lax.rem(chip, n)
    u = y * (1 - c) + z * c
    w = z * (1 - c) + y * c
    partner = a + 1 - 2 * c

    def device_at(uu, ww, cc):
        return ((ww * (1 - cc) + uu * cc) * n + uu * (1 - cc) + ww * cc) * 2 + cc

    def own_index(du, dw):
        return device_at(lax.rem(u + du + n, n), lax.rem(w + dw + n, n), c)

    def partner_index(du, dw):
        return device_at(lax.rem(w + du + n, n), lax.rem(u + dw + n, n), 1 - c)

    neighbour = {("A", 1): own_index(1, 0), ("A", -1): own_index(-1, 0), ("B", 1): own_index(0, 1), ("B", -1): own_index(0, -1)}
    peers = [lax.rem(t + d, tp) for d in range(1, tp)]

    class Gather:
        def __init__(self, number, buffer, own, given, kept):
            self.number, self.buffer, self.own, self.given, self.kept = number, buffer, own, given, kept
            self.half_rows = buffer.shape[1] // 2

        def view(self, index, half=None):
            if half is None:
                return self.buffer.at[index]
            return self.buffer.at[index, pl.ds(half * self.half_rows, self.half_rows)]

        def copy(self, src, dst, group, target):
            return pltpu.make_async_remote_copy(
                src_ref=src, dst_ref=dst, send_sem=send_sem.at[self.number], recv_sem=recv_sem.at[self.number * N_GROUPS + group],
                device_id=(target, t), device_id_type=MESH)

        def ring(self, i):
            axis, sign, source, half, landing = RING[i]
            at = self.own(source)
            to = at if self.own is own_index_of else self.own(landing)
            return self.copy(self.view(at, half), self.view(to, half), RING_GROUP[i], neighbour[axis, sign])

        def push(self, place):
            return self.copy(self.view(self.own(place)), self.view(self.given(place)), len(RING_SHARDS) + PUSH_GROUP[place], partner)

        def shards(self, count, group):
            these = self.buffer.at[pl.ds(0, count)]
            return self.copy(these, these, group, partner)

        def stage(self, name):
            self.arrive(name)
            self.pass_on(name)

        def arrive(self, name):
            group = STAGES[name][0]
            if group is not None:
                self.shards(RING_SHARDS[group], group).wait_recv()

        def pass_on(self, name):
            _, sends, places = STAGES[name]
            for i in sends:
                self.ring(i).start()
            for place in places:
                self.push(place).start()

        def from_partner(self, *groups):
            for group in groups:
                self.shards(len(PUSH_GROUPS[group]), len(RING_SHARDS) + group).wait_recv()

        def drain(self):
            self.shards(ALL_SHARDS, 0).wait_send()

    def own_index_of(place):
        return own_index(*place)

    def chip_slot(place, core):
        return PLACES.index(place) * 2 + core

    by_slot = (OWN_SLOT.get, PARTNER_SLOT.get, PARTNER_SLOT.get)
    by_index = (own_index_of, own_index_of, lambda place: partner_index(*place))
    ks, vs = Gather(0, keys, *by_slot), Gather(1, vals, *by_slot)
    gs, us = Gather(2, gates, *by_index), Gather(3, ups, *by_index)
    downs = Gather(4, dt, lambda place: chip_slot(place, c), lambda place: chip_slot(place[::-1], c),
                   lambda place: chip_slot(place[::-1], 1 - c))

    rows = gate_hbm.shape[0]
    to_gate = pltpu.make_async_copy(gate_hbm, gates.at[a], local_sem.at[0])
    to_up = pltpu.make_async_copy(up_hbm, ups.at[a], local_sem.at[1])
    to_down = pltpu.make_async_copy(down_hbm, dt.at[chip_slot((0, 0), c)], local_sem.at[2])
    to_res = pltpu.make_async_copy(res_hbm, res.at[t], local_sem.at[3])
    to_ow = pltpu.make_async_copy(ow_hbm, ow, local_sem.at[4])
    to_res.start()
    to_gate.start()
    to_up.start()
    to_down.start()
    to_ow.start()

    barrier = pltpu.get_barrier_semaphore()
    for other in [*neighbour.values(), partner]:
        pl.semaphore_signal(barrier, inc=1, device_id=(other, t), device_id_type=MESH)
    for other in peers:
        pl.semaphore_signal(barrier, inc=1, device_id=(a, other), device_id_type=MESH)

    tok = k_ref.shape[0]
    grid_rows = tok // GRID_W

    def table(by_row, by_column):
        mine = by_row[pl.ds(a * grid_rows, grid_rows), :]
        return jnp.concatenate([mine[r:r + 1] + by_column[...] for r in range(grid_rows)], axis=0)

    cosine, sine = table(cos_row, cos_col), table(sin_row, sin_col)
    lane = lax.broadcasted_iota(jnp.int32, cosine.shape, 1)
    low = lax.rem(lax.div(lane, 32), 2) == 0

    def rotated(x, gain):
        x = normalized(x.astype(jnp.float32)) * gain
        swapped = jnp.where(low, pltpu.roll(x, 96, 1), pltpu.roll(x, 32, 1))
        return x * cosine + swapped * sine

    keys[0] = rotated(k_ref[...], kg_ref[...]).astype(jnp.bfloat16)
    for b in range(tok // 128):
        block = v_ref[b * 128:(b + 1) * 128, :].astype(jnp.float32)
        vals[0, b * 128:(b + 1) * 128, :] = block.T.astype(jnp.bfloat16)

    pl.semaphore_wait(barrier, len(neighbour) + 1 + len(peers))
    ks.stage("1A")
    vs.stage("1A")

    def x_copy(src, dst, kind, group, other):
        return pltpu.make_async_remote_copy(src_ref=src, dst_ref=dst, send_sem=x_send.at[kind], recv_sem=x_recv.at[group],
                                            device_id=(a, other), device_id_type=MESH)

    def res_copy(d):
        return x_copy(res.at[t], res.at[t], 0, 0, lax.rem(t + d, tp))

    def att_copy(block, d):
        return x_copy(att.at[block, t], att.at[block, t], 1, 1 + block, lax.rem(t + d, tp))

    def part_copy(half, column, d):
        other = lax.rem(t + d, tp)
        return x_copy(part.at[half, column, other], recv.at[half, column, d - 1], 2 + half, 5 + half * part.shape[1] + column, other)

    def x_all(these, kind, group):
        return x_copy(these, these, kind, group, lax.rem(t + 1, tp))

    to_res.wait()
    for d in range(1, tp):
        res_copy(d).start()

    heads = q_ref.shape[1] // 128
    blocks = tok // 128
    part_rows = 128 // tp
    for h in range(heads):
        rot = rotated(q_ref[:, h * 128:(h + 1) * 128], qg_ref[...]).astype(jnp.bfloat16)
        scaled = rot.astype(jnp.float32) * LOG2_SCALE
        for b in range(blocks):
            turned = jnp.concatenate([scaled[o * 128 + b * part_rows:o * 128 + (b + 1) * part_rows] for o in range(tp)], axis=0).T
            high = turned.astype(jnp.bfloat16)
            at = (b * heads + h) * 128
            qt[0:128, at:at + 128] = high
            qt[128:256, at:at + 128] = (turned - high.astype(jnp.float32)).astype(jnp.bfloat16)

    m_ref[...] = jnp.full_like(m_ref, -1e30)
    l_ref[...] = jnp.zeros_like(l_ref)
    acc[...] = jnp.zeros_like(acc)

    buffers = [s0, s1]

    def columns(j):
        return pl.ds(pl.multiple_of(j * UNIT, UNIT), UNIT)

    def score(chunk, j, into):
        rows_in = keys[pl.ds(chunk * 2, 2)].reshape(2 * tok, 128)
        into[...] = jnp.dot(jnp.concatenate([rows_in, rows_in], axis=1), qt[:, columns(j)], preferred_element_type=jnp.float32)

    def absorb(chunk, j, held):
        turned = jnp.concatenate(
            [vals[chunk * 2 + h, b * 128:(b + 1) * 128, :] for h in range(2) for b in range(blocks)], axis=1)
        at = columns(j)
        scores = held[...]
        before = m_ref[:, at]
        highest = jnp.maximum(before, jnp.max(scores, axis=0, keepdims=True))
        weights = jnp.exp2(scores - highest)
        factor = jnp.exp2(before - highest)
        m_ref[:, at] = highest
        l_ref[:, at] = l_ref[:, at] * factor + jnp.sum(weights, axis=0, keepdims=True)
        acc[:, at] = acc[:, at] * factor + jnp.dot(turned, weights.astype(jnp.bfloat16), preferred_element_type=jnp.float32)

    def both(*groups):
        for gather in (ks, vs):
            gather.from_partner(*groups)

    events = {
        (0, 2): [lambda: ks.stage("1B"), lambda: vs.stage("1B"), lambda: to_down.wait(), lambda: downs.stage("1A"), lambda: ks.stage("2A")],
        (1, 0): [lambda: vs.arrive("2A")],
        (1, 2): [lambda: ks.stage("2B"), lambda: vs.pass_on("2A"), lambda: both(1)],
        (2, 2): [lambda: vs.stage("2B")],
        (3, 2): [lambda: both(2)],
        (4, 0): [lambda: ks.stage("3")],
        (4, 2): [lambda: vs.stage("3")],
        (5, 2): [lambda: to_gate.wait(), lambda: gs.stage("1A")],
        (6, 2): [lambda: ks.stage("4"), lambda: gs.stage("1B")],
        (7, 2): [lambda: both(3)],
    }
    ks.from_partner(0)
    score(0, 0, s0)
    vs.from_partner(0)
    n_units = blocks * heads * 128 // UNIT

    def run(table, index, *unit):
        for at, todo in table.items():
            if at[1:] == unit:
                @pl.when(index == at[0])
                def _():
                    for event in todo:
                        event()

    def first_phase(k, carry):
        for j in range(n_units):
            if j % 2 == 0:
                run(events, k, j)
            if j + 1 < n_units:
                score(k, j + 1, buffers[(j + 1) % 2])
            else:
                score(k + 1, 0, buffers[0])
            absorb(k, j, buffers[j % 2])
        return carry

    lax.fori_loop(0, PHASE1, first_phase, 0)

    last = keys.shape[0] // 2
    later = {
        (0, 8): [lambda: vs.stage("4"), lambda: both(4, 5), lambda: to_up.wait(), lambda: us.stage("1A"), lambda: us.stage("1B")],
        (0, 12): [lambda: both(6, 7), lambda: ks.stage("5"), lambda: gs.stage("2A"), lambda: gs.stage("2B")],
        (0, 14): [lambda: vs.stage("5"), lambda: both(8)],
        (1, 12): [lambda: us.stage("2A"), lambda: us.stage("2B")],
        (2, 10): [lambda: gs.stage("3")],
        (3, 8): [lambda: us.stage("3")],
        (3, 14): [lambda: gs.stage("4"), lambda: downs.stage("1B")],
    }

    def second_phase(j, carry):
        for k in range(PHASE1, last):
            i = k - PHASE1
            if i % 2 == 0:
                run(later, j, k)
            if k + 1 < last:
                score(k + 1, j, buffers[(i + 1) % 2])
            else:
                score(PHASE1, lax.rem(j + 1, n_units), buffers[(i + 1) % 2])
            absorb(k, j, buffers[i % 2])
        at = columns(j)
        mixed = acc[:, at] / l_ref[:, at]
        for h in range(heads):
            att[j, t, :, h * 128:(h + 1) * 128] = mixed[:, h * 128:(h + 1) * 128].T.astype(jnp.bfloat16)
        for d in range(1, tp):
            att_copy(j, d).start()
        return carry

    lax.fori_loop(0, n_units, second_phase, 0)

    to_ow.wait()
    x_all(res.at[pl.ds(0, tp - 1)], 0, 0).wait_recv()


    quarters = 4
    width_part = ow.shape[1] // quarters

    def dots(b, into, i):
        rows_in = jnp.concatenate([att[b, s] for s in range(tp)], axis=1)
        at = slice(i * width_part, (i + 1) * width_part)
        into[:, at] = jnp.dot(rows_in, ow[:, at], preferred_element_type=jnp.float32)

    def norms(b, held, i):
        mine = slice(b * part_rows, (b + 1) * part_rows)
        at = slice(i * part_rows, (i + 1) * part_rows)
        stream = (res[i, mine, :].astype(jnp.float32) + og_ref[...] * normalized(held[at, :])).astype(jnp.bfloat16)
        mid[i, mine, :] = stream
        nrm[b * 128 + i * part_rows:b * 128 + (i + 1) * part_rows, :] = (
            mg_ref[...] * normalized(stream.astype(jnp.float32))).astype(jnp.bfloat16)

    half_rows = tok // 2

    projected = [proj, proj_b]

    def project(first, count, after):
        for b in range(first, first + count + 1):
            now = b < first + count
            if now:
                x_all(att.at[b, pl.ds(0, tp - 1)], 1, 1 + b).wait_recv()
            for i in range(quarters):
                if now:
                    dots(b, projected[b % 2], i)
                if b > first:
                    norms(b - 1, projected[(b - 1) % 2], i)
            for event in after.get((b,), []):
                event()

    width = gates.shape[0] * rows
    n_hidden = gates.shape[2] // 128

    def feed(half, first, last_one):
        these = slice(half * half_rows, (half + 1) * half_rows)

        def gated_dot(i, into):
            at = pl.ds(pl.multiple_of(i * 128, 128), 128)
            pair = jnp.concatenate([gates[:, :, at].reshape(width, 128), ups[:, :, at].reshape(width, 128)], axis=1)
            into[0:half_rows, 0:256] = jnp.dot(nrm[these, :], pair, preferred_element_type=jnp.float32)

        def gating(i, held):
            gate, up = held[0:half_rows, 0:128], held[0:half_rows, 128:256]
            hid[these, pl.ds(pl.multiple_of(i * 128, 128), 128)] = (gate / (1.0 + jnp.exp(-gate)) * up).astype(jnp.bfloat16)

        gated_dot(first, s0)
        pairs = (last_one - first - 1) // 2

        def hidden_pair(i, carry):
            at = first + 2 * i
            gated_dot(at + 1, s1)
            gating(at, s0)
            gated_dot(at + 2, s0)
            gating(at + 1, s1)
            return carry

        lax.fori_loop(0, pairs, hidden_pair, 0)
        at = first + 2 * pairs
        if at + 1 < last_one:
            gated_dot(at + 1, s1)
            gating(at, s0)
            gating(at + 1, s1)
        else:
            gating(at, s0)

    per_block = 256 // rows
    n_columns = dt.shape[0] // per_block
    owned = half_rows // tp

    def shrink(half, first, count, before):
        these = slice(half * half_rows, (half + 1) * half_rows)

        def down_block(i, carry):
            run(before, i)
            weight = dt[pl.ds(i * per_block, per_block)].reshape(256, dt.shape[2])
            share = lax.dot_general(hid[these, :], weight, (((1,), (1,)), ((), ())), preferred_element_type=jnp.float32).astype(jnp.bfloat16)
            for o in range(tp):
                part[half, i, o] = jnp.concatenate(
                    [share[b * 128 + o * part_rows:b * 128 + (o + 1) * part_rows] for b in range(blocks // 2)], axis=0)

            @pl.when(i > first)
            def _():
                for d in range(1, tp):
                    part_copy(half, i - 1, d).start()
            return carry

        lax.fori_loop(first, first + count, down_block, 0)
        for d in range(1, tp):
            part_copy(half, first + count - 1, d).start()

    project(0, blocks - 1, {(1,): [lambda: us.stage("4"), lambda: downs.stage("2A")],
                        (2,): [lambda: downs.stage("2B"), lambda: gs.stage("5")],
                        (3,): [lambda: us.stage("5")]})
    for gather in (gs, us):
        gather.from_partner(*range(len(PUSH_GROUPS)))
    feed(0, 0, n_hidden)
    downs.from_partner(0, 1, 2)
    shrink(0, 0, 2, {})
    downs.stage("3")
    project(blocks - 1, 1, {})
    downs.from_partner(3, 4, 5)
    shrink(0, 2, 3, {})
    feed(1, 0, n_hidden)
    shrink(1, 0, 2, {})
    downs.stage("4")
    shrink(1, 2, 3, {})
    downs.from_partner(6, 7)
    downs.stage("5")
    shrink(0, 5, 2, {})
    shrink(1, 5, 2, {})
    downs.from_partner(8)
    shrink(0, 7, 1, {})
    shrink(1, 7, 1, {})

    for half, columns_of in ((0, range(5)), (1, range(5)), (0, [5, 6]), (1, [5, 6]), (0, [7]), (1, [7])):
        for i in columns_of:
            x_all(recv.at[half, i], 2, 5 + half * n_columns + i).wait_recv()
            total = part[half, i, t].astype(jnp.float32)
            for d in range(tp - 1):
                total = total + recv[half, i, d].astype(jnp.float32)
            for h in range(2):
                chip_at = lax.div(own_index(*PLACES[2 * i + h]), 2)
                proj[half * owned:(half + 1) * owned, pl.ds(pl.multiple_of(chip_at * 128, 128), 128)] = total[:, h * 128:(h + 1) * 128]

    def finish(i, carry):
        at = pl.ds(pl.multiple_of(i * 32, 32), 32)
        out_ref[at, :] = (mid[t, at, :].astype(jnp.float32) + fg_ref[...] * normalized(proj[at, :])).astype(jnp.bfloat16)
        return carry

    lax.fori_loop(0, 4, finish, 0)

    for gather in (ks, vs, gs, us, downs):
        gather.drain()
    x_all(res.at[pl.ds(0, tp - 1)], 0, 0).wait_send()
    x_all(att.at[pl.ds(0, tp - 1)], 1, 0).wait_send()
    for half in range(2):
        x_all(part.at[half, pl.ds(0, n_columns * (tp - 1) // tp)], 2 + half, 0).wait_send()


def on_device(queries, keys, values, q_gain, k_gain, out_weight, out_gain, residual_in, mlp_gain, gate_weight, up_weight, down_weight, final_gain):
    sp, tp = lax.axis_size("sp"), lax.axis_size("tp")
    n = math.isqrt(sp // 2)
    tok, head = keys.shape
    rows, hidden = gate_weight.shape
    width = out_weight.shape[1]
    quarter = head // 4
    freqs = np.float32(10000.0) ** (-np.arange(quarter, dtype=np.float32) / np.float32(quarter))

    def table(function, signs, count, low):
        angle = np.arange(count, dtype=np.float32)[:, None] * freqs
        values, empty = function(angle.astype(np.float64)).astype(np.float32), np.zeros((count, 2 * quarter), np.float32)
        turned = np.concatenate([signs[0] * values, signs[1] * values], axis=1)
        return jnp.asarray(np.concatenate([turned, empty] if low else [empty, turned], axis=1).astype(np.float32))

    tables = [table(function, signs, count, low) for function, signs in ((np.cos, (1.0, 1.0)), (np.sin, (-1.0, 1.0)))
              for count, low in ((sp * tok // GRID_W, True), (GRID_W, False))]
    blocks = tok // 128
    bf16, f32 = jnp.bfloat16, jnp.float32
    vmem = pl.BlockSpec(memory_space=pltpu.VMEM)
    anywhere = pl.BlockSpec(memory_space=pl.ANY)
    n_columns = width // 256
    q_columns = tok * queries.shape[1] // head
    return pl.pallas_call(
        functools.partial(layer_kernel, n, tp),
        out_shape=jax.ShapeDtypeStruct(residual_in.shape, bf16),
        in_specs=[vmem] * 12 + [anywhere] * 5,
        out_specs=vmem,
        scratch_shapes=[
            pltpu.VMEM((sp, tok, head), bf16),
            pltpu.VMEM((sp, tok, head), bf16),
            pltpu.VMEM((sp, rows, hidden), bf16),
            pltpu.VMEM((sp, rows, hidden), bf16),
            pltpu.VMEM((sp, rows, hidden), bf16),
            pltpu.VMEM(out_weight.shape, bf16),
            pltpu.VMEM((tp, *residual_in.shape), bf16),
            pltpu.VMEM((blocks, tp, 128, queries.shape[1]), bf16),
            pltpu.VMEM((blocks, 128, width), bf16),
            pltpu.VMEM((tok, width), bf16),
            pltpu.VMEM((tok, hidden), bf16),
            pltpu.VMEM((2, n_columns, tp, 64, 256), bf16),
            pltpu.VMEM((2, n_columns, tp - 1, 64, 256), bf16),
            pltpu.VMEM((128, width), f32),
            pltpu.VMEM((128, width), f32),
            pltpu.VMEM((2 * head, q_columns), bf16),
            pltpu.VMEM((2 * tok, UNIT), f32),
            pltpu.VMEM((2 * tok, UNIT), f32),
            pltpu.VMEM((head, q_columns), f32),
            pltpu.VMEM((1, q_columns), f32),
            pltpu.VMEM((1, q_columns), f32),
            pltpu.SemaphoreType.DMA((5,)),
            pltpu.SemaphoreType.DMA((5 * N_GROUPS,)),
            pltpu.SemaphoreType.DMA((4,)),
            pltpu.SemaphoreType.DMA((5 + 2 * n_columns,)),
            pltpu.SemaphoreType.DMA((5,)),
        ],
        compiler_params=pltpu.CompilerParams(collective_id=0, has_side_effects=True, vmem_limit_bytes=67043328),
        name="layer",
    )(queries, keys, values, *tables,
      q_gain[None], k_gain[None], out_gain[None], mlp_gain[None], final_gain[None],
      out_weight, residual_in, gate_weight, up_weight, down_weight.T)


def solution(mesh):
    return jax.shard_map(
        on_device,
        mesh=mesh,
        in_specs=(
            P("sp", "tp"), P("sp", "tp"), P("sp", "tp"), P(), P(), P(), P(), P(("sp", "tp"), None), P(),
            P("sp", "tp"), P("sp", "tp"), P("tp", "sp"), P(),
        ),
        out_specs=P(("sp", "tp"), None),
        check_vma=False,
    )
```

```python
import functools
import math

import jax
import jax.numpy as jnp
import numpy as np
from jax import lax
from jax.experimental import pallas as pl
from jax.experimental.pallas import tpu as pltpu
from jax.sharding import PartitionSpec as P

GRID_W = 64
MESH = pl.DeviceIdType.MESH
EPS = 1e-06
LOG2_SCALE = 128 ** (-0.5) * math.log2(math.e)
UNIT = 512
PHASE1 = 8

RING = [
    ("A", 1, (0, 0), None, (-1, 0)),
    ("A", -1, (0, 0), None, (1, 0)),
    ("B", 1, (0, 0), None, (0, -1)),
    ("B", -1, (0, 0), None, (0, 1)),
    ("A", 1, (-1, 0), 0, (2, 0)),
    ("A", -1, (1, 0), 1, (2, 0)),
    ("B", 1, (-1, 0), None, (-1, -1)),
    ("B", -1, (-1, 0), None, (-1, 1)),
    ("B", 1, (1, 0), None, (1, -1)),
    ("B", -1, (1, 0), None, (1, 1)),
    ("B", 1, (0, -1), 0, (0, 2)),
    ("B", -1, (0, 1), 1, (0, 2)),
    ("B", 1, (2, 0), None, (2, -1)),
    ("B", -1, (2, 0), None, (2, 1)),
    ("B", 1, (-1, -1), 0, (-1, 2)),
    ("B", -1, (-1, 1), 1, (-1, 2)),
    ("B", 1, (1, -1), 0, (1, 2)),
    ("B", -1, (1, 1), 1, (1, 2)),
    ("B", 1, (2, -1), 0, (2, 2)),
    ("B", -1, (2, 1), 1, (2, 2)),
]
PLACES = [(0, 0), (-1, 0), (1, 0), (0, -1), (0, 1), (2, 0), (0, 2), (-1, -1), (-1, 1), (1, -1), (1, 1), (2, -1), (2, 1), (-1, 2), (1, 2), (2, 2)]
STAGES = {
    "1A": (None, [0, 1], [(0, 0)]),
    "1B": (None, [2, 3], []),
    "2A": (0, [4, 5, 6, 7, 8, 9], [(-1, 0), (1, 0)]),
    "2B": (1, [10, 11], [(0, -1), (0, 1)]),
    "3": (2, [12, 13, 14, 15, 16, 17], [(2, 0), (0, 2), (-1, -1), (-1, 1), (1, -1), (1, 1)]),
    "4": (3, [18, 19], [(2, -1), (2, 1), (-1, 2), (1, 2)]),
    "5": (4, [], [(2, 2)]),
}
RING_GROUPS = [[0, 1], [2, 3], [4, 5, 6, 7, 8, 9, 10, 11], [12, 13, 14, 15, 16, 17], [18, 19]]
OWN_SLOT = {(0, 0): 0, (-1, 0): 2, (1, 0): 3, (0, -1): 6, (0, 1): 7, (2, 0): 10, (0, 2): 11, (-1, -1): 12, (-1, 1): 13, (1, -1): 14, (1, 1): 15,
            (2, -1): 22, (2, 1): 23, (-1, 2): 24, (1, 2): 25, (2, 2): 30}
PARTNER_SLOT = {(0, 0): 1, (-1, 0): 4, (1, 0): 5, (0, -1): 8, (0, 1): 9, (2, 0): 16, (0, 2): 17, (-1, -1): 18, (-1, 1): 19, (1, -1): 20, (1, 1): 21,
                (2, -1): 26, (2, 1): 27, (-1, 2): 28, (1, 2): 29, (2, 2): 31}
RING_GROUP = {i: number for number, group in enumerate(RING_GROUPS) for i in group}
RING_SHARDS = [sum(2 if RING[i][3] is None else 1 for i in group) // 2 for group in RING_GROUPS]
PUSH_GROUPS = [PLACES[0:1], PLACES[1:3], PLACES[3:5], PLACES[5:7], PLACES[7:9], PLACES[9:11], PLACES[11:13], PLACES[13:15], PLACES[15:16]]
PUSH_GROUP = {place: number for number, group in enumerate(PUSH_GROUPS) for place in group}
N_GROUPS = len(RING_SHARDS) + len(PUSH_GROUPS)
ALL_SHARDS = sum(RING_SHARDS) + len(PLACES)


def normalized(x):
    return x * lax.rsqrt(jnp.mean(x * x, axis=-1, keepdims=True) + EPS)


def layer_kernel(n, tp, q_ref, k_ref, v_ref, cos_row, cos_col, sin_row, sin_col, qg_ref, kg_ref, og_ref, mg_ref, fg_ref,
                 ow_hbm, res_hbm, gate_hbm, up_hbm, down_hbm, out_ref,
                 keys, vals, gates, ups, dt, ow, res, att, mid, nrm, hid, part, recv, proj, proj_b, qt, s0, s1, acc, m_ref, l_ref,
                 send_sem, recv_sem, x_send, x_recv, local_sem):
    a = lax.axis_index("sp")
    t = lax.axis_index("tp")
    c = lax.rem(a, 2)
    chip = lax.div(a, 2)
    z = lax.div(chip, n)
    y = lax.rem(chip, n)
    u = y * (1 - c) + z * c
    w = z * (1 - c) + y * c
    partner = a + 1 - 2 * c

    def device_at(uu, ww, cc):
        return ((ww * (1 - cc) + uu * cc) * n + uu * (1 - cc) + ww * cc) * 2 + cc

    def own_index(du, dw):
        return device_at(lax.rem(u + du + n, n), lax.rem(w + dw + n, n), c)

    def partner_index(du, dw):
        return device_at(lax.rem(w + du + n, n), lax.rem(u + dw + n, n), 1 - c)

    neighbour = {("A", 1): own_index(1, 0), ("A", -1): own_index(-1, 0), ("B", 1): own_index(0, 1), ("B", -1): own_index(0, -1)}
    peers = [lax.rem(t + d, tp) for d in range(1, tp)]
    far_first = sorted(range(1, tp), key=lambda d: -min(d, tp - d))

    class Gather:
        def __init__(self, number, buffer, own, given, kept):
            self.number, self.buffer, self.own, self.given, self.kept = number, buffer, own, given, kept
            self.half_rows = buffer.shape[1] // 2

        def view(self, index, half=None):
            if half is None:
                return self.buffer.at[index]
            return self.buffer.at[index, pl.ds(half * self.half_rows, self.half_rows)]

        def copy(self, src, dst, group, target):
            return pltpu.make_async_remote_copy(
                src_ref=src, dst_ref=dst, send_sem=send_sem.at[self.number], recv_sem=recv_sem.at[self.number * N_GROUPS + group],
                device_id=(target, t), device_id_type=MESH)

        def ring(self, i):
            axis, sign, source, half, landing = RING[i]
            at = self.own(source)
            to = at if self.own is own_index_of else self.own(landing)
            return self.copy(self.view(at, half), self.view(to, half), RING_GROUP[i], neighbour[axis, sign])

        def push(self, place):
            return self.copy(self.view(self.own(place)), self.view(self.given(place)), len(RING_SHARDS) + PUSH_GROUP[place], partner)

        def shards(self, count, group):
            these = self.buffer.at[pl.ds(0, count)]
            return self.copy(these, these, group, partner)

        def stage(self, name):
            self.arrive(name)
            self.pass_on(name)

        def arrive(self, name):
            group = STAGES[name][0]
            if group is not None:
                self.shards(RING_SHARDS[group], group).wait_recv()

        def pass_on(self, name):
            _, sends, places = STAGES[name]
            for i in sends:
                self.ring(i).start()
            for place in places:
                self.push(place).start()

        def from_partner(self, *groups):
            for group in groups:
                self.shards(len(PUSH_GROUPS[group]), len(RING_SHARDS) + group).wait_recv()

        def drain(self):
            self.shards(ALL_SHARDS, 0).wait_send()

    def own_index_of(place):
        return own_index(*place)

    def chip_slot(place, core):
        return PLACES.index(place) * 2 + core

    by_slot = (OWN_SLOT.get, PARTNER_SLOT.get, PARTNER_SLOT.get)
    by_index = (own_index_of, own_index_of, lambda place: partner_index(*place))
    ks, vs = Gather(0, keys, *by_slot), Gather(1, vals, *by_slot)
    gs, us = Gather(2, gates, *by_index), Gather(3, ups, *by_index)
    downs = Gather(4, dt, lambda place: chip_slot(place, c), lambda place: chip_slot(place[::-1], c),
                   lambda place: chip_slot(place[::-1], 1 - c))

    rows = gate_hbm.shape[0]
    to_gate = pltpu.make_async_copy(gate_hbm, gates.at[a], local_sem.at[0])
    to_up = pltpu.make_async_copy(up_hbm, ups.at[a], local_sem.at[1])
    to_down = pltpu.make_async_copy(down_hbm, dt.at[chip_slot((0, 0), c)], local_sem.at[2])
    to_res = pltpu.make_async_copy(res_hbm, res.at[t], local_sem.at[3])
    to_ow = pltpu.make_async_copy(ow_hbm, ow, local_sem.at[4])
    to_res.start()
    to_gate.start()
    to_up.start()
    to_down.start()
    to_ow.start()

    barrier = pltpu.get_barrier_semaphore()
    for other in [*neighbour.values(), partner]:
        pl.semaphore_signal(barrier, inc=1, device_id=(other, t), device_id_type=MESH)
    for other in peers:
        pl.semaphore_signal(barrier, inc=1, device_id=(a, other), device_id_type=MESH)

    tok = k_ref.shape[0]
    grid_rows = tok // GRID_W

    def table(by_row, by_column):
        mine = by_row[pl.ds(a * grid_rows, grid_rows), :]
        return jnp.concatenate([mine[r:r + 1] + by_column[...] for r in range(grid_rows)], axis=0)

    cosine, sine = table(cos_row, cos_col), table(sin_row, sin_col)
    lane = lax.broadcasted_iota(jnp.int32, cosine.shape, 1)
    low = lax.rem(lax.div(lane, 32), 2) == 0

    def rotated(x, gain):
        x = normalized(x.astype(jnp.float32)) * gain
        swapped = jnp.where(low, pltpu.roll(x, 96, 1), pltpu.roll(x, 32, 1))
        return x * cosine + swapped * sine

    keys[0] = rotated(k_ref[...], kg_ref[...]).astype(jnp.bfloat16)
    for b in range(tok // 128):
        block = v_ref[b * 128:(b + 1) * 128, :].astype(jnp.float32)
        vals[0, b * 128:(b + 1) * 128, :] = block.T.astype(jnp.bfloat16)

    pl.semaphore_wait(barrier, len(neighbour) + 1 + len(peers))
    ks.stage("1A")
    vs.stage("1A")

    def x_copy(src, dst, kind, group, other):
        return pltpu.make_async_remote_copy(src_ref=src, dst_ref=dst, send_sem=x_send.at[kind], recv_sem=x_recv.at[group],
                                            device_id=(a, other), device_id_type=MESH)

    def res_copy(d):
        return x_copy(res.at[t], res.at[t], 0, 0, lax.rem(t + d, tp))

    def att_copy(block, d):
        return x_copy(att.at[block, t], att.at[block, t], 1, 1 + block, lax.rem(t + d, tp))

    def part_copy(half, column, d):
        other = lax.rem(t + d, tp)
        return x_copy(part.at[half, column, other], recv.at[half, column, d - 1], 2 + half, 5 + half * part.shape[1] + column, other)

    def x_all(these, kind, group):
        return x_copy(these, these, kind, group, lax.rem(t + 1, tp))

    to_res.wait()
    for d in range(1, tp):
        res_copy(d).start()

    heads = q_ref.shape[1] // 128
    blocks = tok // 128
    part_rows = 128 // tp
    for h in range(heads):
        rot = rotated(q_ref[:, h * 128:(h + 1) * 128], qg_ref[...]).astype(jnp.bfloat16)
        scaled = rot.astype(jnp.float32) * LOG2_SCALE
        for b in range(blocks):
            turned = jnp.concatenate([scaled[o * 128 + b * part_rows:o * 128 + (b + 1) * part_rows] for o in range(tp)], axis=0).T
            high = turned.astype(jnp.bfloat16)
            at = (b * heads + h) * 128
            qt[0:128, at:at + 128] = high
            qt[128:256, at:at + 128] = (turned - high.astype(jnp.float32)).astype(jnp.bfloat16)

    m_ref[...] = jnp.full_like(m_ref, -1e30)
    l_ref[...] = jnp.zeros_like(l_ref)
    acc[...] = jnp.zeros_like(acc)

    buffers = [s0, s1]

    def columns(j):
        return pl.ds(pl.multiple_of(j * UNIT, UNIT), UNIT)

    def score(chunk, j, into):
        rows_in = keys[pl.ds(chunk * 2, 2)].reshape(2 * tok, 128)
        into[...] = jnp.dot(jnp.concatenate([rows_in, rows_in], axis=1), qt[:, columns(j)], preferred_element_type=jnp.float32)

    def absorb(chunk, j, held):
        turned = jnp.concatenate(
            [vals[chunk * 2 + h, b * 128:(b + 1) * 128, :] for h in range(2) for b in range(blocks)], axis=1)
        at = columns(j)
        scores = held[...]
        before = m_ref[:, at]
        highest = jnp.maximum(before, jnp.max(scores, axis=0, keepdims=True))
        weights = jnp.exp2(scores - highest)
        factor = jnp.exp2(before - highest)
        m_ref[:, at] = highest
        l_ref[:, at] = l_ref[:, at] * factor + jnp.sum(weights, axis=0, keepdims=True)
        acc[:, at] = acc[:, at] * factor + jnp.dot(turned, weights.astype(jnp.bfloat16), preferred_element_type=jnp.float32)

    def both(*groups):
        for gather in (ks, vs):
            gather.from_partner(*groups)

    events = {
        (0, 2): [lambda: ks.stage("1B"), lambda: vs.stage("1B"), lambda: to_down.wait(), lambda: downs.stage("1A"), lambda: ks.stage("2A")],
        (1, 0): [lambda: vs.arrive("2A")],
        (1, 2): [lambda: ks.stage("2B"), lambda: vs.pass_on("2A"), lambda: both(1)],
        (2, 2): [lambda: vs.stage("2B")],
        (3, 2): [lambda: both(2)],
        (4, 0): [lambda: ks.stage("3"), lambda: to_gate.wait(), lambda: gs.stage("1A")],
        (4, 2): [lambda: vs.stage("3")],
        (5, 2): [lambda: gs.stage("1B")],
        (6, 2): [lambda: ks.stage("4"), lambda: to_up.wait(), lambda: us.stage("1A")],
        (7, 2): [lambda: both(3)],
    }
    ks.from_partner(0)
    score(0, 0, s0)
    vs.from_partner(0)
    n_units = blocks * heads * 128 // UNIT

    def run(table, index, *unit):
        for at, todo in table.items():
            if at[1:] == unit:
                @pl.when(index == at[0])
                def _():
                    for event in todo:
                        event()

    def first_phase(k, carry):
        for j in range(n_units):
            if j % 2 == 0:
                run(events, k, j)
            if j + 1 < n_units:
                score(k, j + 1, buffers[(j + 1) % 2])
            else:
                score(k + 1, 0, buffers[0])
            absorb(k, j, buffers[j % 2])
        return carry

    lax.fori_loop(0, PHASE1, first_phase, 0)

    last = keys.shape[0] // 2
    later = {
        (0, 8): [lambda: vs.stage("4"), lambda: both(4, 5), lambda: us.stage("1B")],
        (0, 10): [lambda: gs.stage("2A"), lambda: gs.stage("2B")],
        (0, 12): [lambda: both(6, 7), lambda: ks.stage("5")],
        (0, 14): [lambda: vs.stage("5"), lambda: both(8)],
        (1, 10): [lambda: us.stage("2A"), lambda: us.stage("2B")],
        (2, 8): [lambda: gs.stage("3")],
        (3, 8): [lambda: us.stage("3")],
        (3, 14): [lambda: gs.stage("4"), lambda: downs.stage("1B")],
    }

    def second_phase(j, carry):
        for k in range(PHASE1, last):
            i = k - PHASE1
            if i % 2 == 0:
                run(later, j, k)
            if k + 1 < last:
                score(k + 1, j, buffers[(i + 1) % 2])
            else:
                score(PHASE1, lax.rem(j + 1, n_units), buffers[(i + 1) % 2])
            absorb(k, j, buffers[i % 2])
        at = columns(j)
        mixed = acc[:, at] / l_ref[:, at]
        for h in range(heads):
            att[j, t, :, h * 128:(h + 1) * 128] = mixed[:, h * 128:(h + 1) * 128].T.astype(jnp.bfloat16)
        for d in far_first:
            att_copy(j, d).start()
        return carry

    lax.fori_loop(0, n_units, second_phase, 0)

    to_ow.wait()
    x_all(res.at[pl.ds(0, tp - 1)], 0, 0).wait_recv()


    quarters = 4
    width_part = ow.shape[1] // quarters

    def dots(b, into, i):
        rows_in = jnp.concatenate([att[b, s] for s in range(tp)], axis=1)
        at = slice(i * width_part, (i + 1) * width_part)
        into[:, at] = jnp.dot(rows_in, ow[:, at], preferred_element_type=jnp.float32)

    def norms(b, held, i):
        mine = slice(b * part_rows, (b + 1) * part_rows)
        at = slice(i * part_rows, (i + 1) * part_rows)
        stream = (res[i, mine, :].astype(jnp.float32) + og_ref[...] * normalized(held[at, :])).astype(jnp.bfloat16)
        mid[i, mine, :] = stream
        nrm[b * 128 + i * part_rows:b * 128 + (i + 1) * part_rows, :] = (
            mg_ref[...] * normalized(stream.astype(jnp.float32))).astype(jnp.bfloat16)

    half_rows = tok // 2

    projected = [proj, proj_b]

    def project(first, count, after):
        for b in range(first, first + count + 1):
            now = b < first + count
            if now:
                x_all(att.at[b, pl.ds(0, tp - 1)], 1, 1 + b).wait_recv()
            for i in range(quarters):
                if now:
                    dots(b, projected[b % 2], i)
                if b > first:
                    norms(b - 1, projected[(b - 1) % 2], i)
            for event in after.get((b,), []):
                event()

    width = gates.shape[0] * rows
    n_hidden = gates.shape[2] // 128

    def feed(half, first, last_one):
        these = slice(half * half_rows, (half + 1) * half_rows)

        def gated_dot(i, into):
            at = pl.ds(pl.multiple_of(i * 128, 128), 128)
            pair = jnp.concatenate([gates[:, :, at].reshape(width, 128), ups[:, :, at].reshape(width, 128)], axis=1)
            into[0:half_rows, 0:256] = jnp.dot(nrm[these, :], pair, preferred_element_type=jnp.float32)

        def gating(i, held):
            gate, up = held[0:half_rows, 0:128], held[0:half_rows, 128:256]
            hid[these, pl.ds(pl.multiple_of(i * 128, 128), 128)] = (gate / (1.0 + jnp.exp(-gate)) * up).astype(jnp.bfloat16)

        gated_dot(first, s0)
        pairs = (last_one - first - 1) // 2

        def hidden_pair(i, carry):
            at = first + 2 * i
            gated_dot(at + 1, s1)
            gating(at, s0)
            gated_dot(at + 2, s0)
            gating(at + 1, s1)
            return carry

        lax.fori_loop(0, pairs, hidden_pair, 0)
        at = first + 2 * pairs
        if at + 1 < last_one:
            gated_dot(at + 1, s1)
            gating(at, s0)
            gating(at + 1, s1)
        else:
            gating(at, s0)

    per_block = 256 // rows
    n_columns = dt.shape[0] // per_block
    owned = half_rows // tp

    def shrink(half, first, count, before):
        these = slice(half * half_rows, (half + 1) * half_rows)

        def down_block(i, carry):
            run(before, i)
            weight = dt[pl.ds(i * per_block, per_block)].reshape(256, dt.shape[2])
            share = lax.dot_general(hid[these, :], weight, (((1,), (1,)), ((), ())), preferred_element_type=jnp.float32).astype(jnp.bfloat16)
            for o in range(tp):
                part[half, i, o] = jnp.concatenate(
                    [share[b * 128 + o * part_rows:b * 128 + (o + 1) * part_rows] for b in range(blocks // 2)], axis=0)

            @pl.when(i > first)
            def _():
                for d in far_first:
                    part_copy(half, i - 1, d).start()
            return carry

        lax.fori_loop(first, first + count, down_block, 0)
        for d in far_first:
            part_copy(half, first + count - 1, d).start()

    project(0, blocks - 1, {(0,): [lambda: us.stage("4"), lambda: downs.stage("2A")],
                        (2,): [lambda: downs.stage("2B"), lambda: gs.stage("5")],
                        (3,): [lambda: us.stage("5")]})
    for gather in (gs, us):
        gather.from_partner(*range(len(PUSH_GROUPS)))
    feed(0, 0, n_hidden)
    downs.from_partner(0, 1, 2)
    shrink(0, 0, 2, {})
    downs.stage("3")
    project(blocks - 1, 1, {})
    downs.from_partner(3, 4, 5)
    shrink(0, 2, 3, {})
    feed(1, 0, n_hidden)
    shrink(1, 0, 2, {})
    downs.stage("4")
    shrink(1, 2, 3, {})
    downs.from_partner(6, 7)
    downs.stage("5")
    shrink(0, 5, 2, {})
    shrink(1, 5, 2, {})
    downs.from_partner(8)
    shrink(0, 7, 1, {})
    shrink(1, 7, 1, {})

    for half, columns_of in ((0, range(5)), (1, range(5)), (0, [5, 6]), (1, [5, 6]), (0, [7]), (1, [7])):
        for i in columns_of:
            x_all(recv.at[half, i], 2, 5 + half * n_columns + i).wait_recv()
            total = part[half, i, t].astype(jnp.float32)
            for d in range(tp - 1):
                total = total + recv[half, i, d].astype(jnp.float32)
            for h in range(2):
                chip_at = lax.div(own_index(*PLACES[2 * i + h]), 2)
                proj[half * owned:(half + 1) * owned, pl.ds(pl.multiple_of(chip_at * 128, 128), 128)] = total[:, h * 128:(h + 1) * 128]

    def finish(i, carry):
        at = pl.ds(pl.multiple_of(i * 32, 32), 32)
        out_ref[at, :] = (mid[t, at, :].astype(jnp.float32) + fg_ref[...] * normalized(proj[at, :])).astype(jnp.bfloat16)
        return carry

    lax.fori_loop(0, 4, finish, 0)

    for gather in (ks, vs, gs, us, downs):
        gather.drain()
    x_all(res.at[pl.ds(0, tp - 1)], 0, 0).wait_send()
    x_all(att.at[pl.ds(0, tp - 1)], 1, 0).wait_send()
    for half in range(2):
        x_all(part.at[half, pl.ds(0, n_columns * (tp - 1) // tp)], 2 + half, 0).wait_send()


def on_device(queries, keys, values, q_gain, k_gain, out_weight, out_gain, residual_in, mlp_gain, gate_weight, up_weight, down_weight, final_gain):
    sp, tp = lax.axis_size("sp"), lax.axis_size("tp")
    n = math.isqrt(sp // 2)
    tok, head = keys.shape
    rows, hidden = gate_weight.shape
    width = out_weight.shape[1]
    quarter = head // 4
    freqs = np.float32(10000.0) ** (-np.arange(quarter, dtype=np.float32) / np.float32(quarter))

    def table(function, signs, count, low):
        angle = np.arange(count, dtype=np.float32)[:, None] * freqs
        values, empty = function(angle.astype(np.float64)).astype(np.float32), np.zeros((count, 2 * quarter), np.float32)
        turned = np.concatenate([signs[0] * values, signs[1] * values], axis=1)
        return jnp.asarray(np.concatenate([turned, empty] if low else [empty, turned], axis=1).astype(np.float32))

    tables = [table(function, signs, count, low) for function, signs in ((np.cos, (1.0, 1.0)), (np.sin, (-1.0, 1.0)))
              for count, low in ((sp * tok // GRID_W, True), (GRID_W, False))]
    blocks = tok // 128
    bf16, f32 = jnp.bfloat16, jnp.float32
    vmem = pl.BlockSpec(memory_space=pltpu.VMEM)
    anywhere = pl.BlockSpec(memory_space=pl.ANY)
    n_columns = width // 256
    q_columns = tok * queries.shape[1] // head
    return pl.pallas_call(
        functools.partial(layer_kernel, n, tp),
        out_shape=jax.ShapeDtypeStruct(residual_in.shape, bf16),
        in_specs=[vmem] * 12 + [anywhere] * 5,
        out_specs=vmem,
        scratch_shapes=[
            pltpu.VMEM((sp, tok, head), bf16),
            pltpu.VMEM((sp, tok, head), bf16),
            pltpu.VMEM((sp, rows, hidden), bf16),
            pltpu.VMEM((sp, rows, hidden), bf16),
            pltpu.VMEM((sp, rows, hidden), bf16),
            pltpu.VMEM(out_weight.shape, bf16),
            pltpu.VMEM((tp, *residual_in.shape), bf16),
            pltpu.VMEM((blocks, tp, 128, queries.shape[1]), bf16),
            pltpu.VMEM((blocks, 128, width), bf16),
            pltpu.VMEM((tok, width), bf16),
            pltpu.VMEM((tok, hidden), bf16),
            pltpu.VMEM((2, n_columns, tp, 64, 256), bf16),
            pltpu.VMEM((2, n_columns, tp - 1, 64, 256), bf16),
            pltpu.VMEM((128, width), f32),
            pltpu.VMEM((128, width), f32),
            pltpu.VMEM((2 * head, q_columns), bf16),
            pltpu.VMEM((2 * tok, UNIT), f32),
            pltpu.VMEM((2 * tok, UNIT), f32),
            pltpu.VMEM((head, q_columns), f32),
            pltpu.VMEM((1, q_columns), f32),
            pltpu.VMEM((1, q_columns), f32),
            pltpu.SemaphoreType.DMA((5,)),
            pltpu.SemaphoreType.DMA((5 * N_GROUPS,)),
            pltpu.SemaphoreType.DMA((4,)),
            pltpu.SemaphoreType.DMA((5 + 2 * n_columns,)),
            pltpu.SemaphoreType.DMA((5,)),
        ],
        compiler_params=pltpu.CompilerParams(collective_id=0, has_side_effects=True, vmem_limit_bytes=67043328),
        name="layer",
    )(queries, keys, values, *tables,
      q_gain[None], k_gain[None], out_gain[None], mlp_gain[None], final_gain[None],
      out_weight, residual_in, gate_weight, up_weight, down_weight.T)


def solution(mesh):
    return jax.shard_map(
        on_device,
        mesh=mesh,
        in_specs=(
            P("sp", "tp"), P("sp", "tp"), P("sp", "tp"), P(), P(), P(), P(), P(("sp", "tp"), None), P(),
            P("sp", "tp"), P("sp", "tp"), P("tp", "sp"), P(),
        ),
        out_specs=P(("sp", "tp"), None),
        check_vma=False,
    )
```

```python
import functools
import math

import jax
import jax.numpy as jnp
import numpy as np
from jax import lax
from jax.experimental import pallas as pl
from jax.experimental.pallas import tpu as pltpu
from jax.sharding import PartitionSpec as P

GRID_W = 64
MESH = pl.DeviceIdType.MESH
EPS = 1e-06
LOG2_SCALE = 128 ** (-0.5) * math.log2(math.e)
UNIT = 512
PHASE1 = 8

RING = [
    ("A", 1, (0, 0), None, (-1, 0)),
    ("A", -1, (0, 0), None, (1, 0)),
    ("B", 1, (0, 0), None, (0, -1)),
    ("B", -1, (0, 0), None, (0, 1)),
    ("A", 1, (-1, 0), 0, (2, 0)),
    ("A", -1, (1, 0), 1, (2, 0)),
    ("B", 1, (-1, 0), None, (-1, -1)),
    ("B", -1, (-1, 0), None, (-1, 1)),
    ("B", 1, (1, 0), None, (1, -1)),
    ("B", -1, (1, 0), None, (1, 1)),
    ("B", 1, (0, -1), 0, (0, 2)),
    ("B", -1, (0, 1), 1, (0, 2)),
    ("B", 1, (2, 0), None, (2, -1)),
    ("B", -1, (2, 0), None, (2, 1)),
    ("B", 1, (-1, -1), 0, (-1, 2)),
    ("B", -1, (-1, 1), 1, (-1, 2)),
    ("B", 1, (1, -1), 0, (1, 2)),
    ("B", -1, (1, 1), 1, (1, 2)),
    ("B", 1, (2, -1), 0, (2, 2)),
    ("B", -1, (2, 1), 1, (2, 2)),
]
PLACES = [(0, 0), (-1, 0), (1, 0), (0, -1), (0, 1), (2, 0), (0, 2), (-1, -1), (-1, 1), (1, -1), (1, 1), (2, -1), (2, 1), (-1, 2), (1, 2), (2, 2)]
STAGES = {
    "1A": (None, [0, 1], [(0, 0)]),
    "1B": (None, [2, 3], []),
    "2A": (0, [4, 5, 6, 7, 8, 9], [(-1, 0), (1, 0)]),
    "2B": (1, [10, 11], [(0, -1), (0, 1)]),
    "3": (2, [12, 13, 14, 15, 16, 17], [(2, 0), (0, 2), (-1, -1), (-1, 1), (1, -1), (1, 1)]),
    "4": (3, [18, 19], [(2, -1), (2, 1), (-1, 2), (1, 2)]),
    "5": (4, [], [(2, 2)]),
}
RING_GROUPS = [[0, 1], [2, 3], [4, 5, 6, 7, 8, 9, 10, 11], [12, 13, 14, 15, 16, 17], [18, 19]]
OWN_SLOT = {(0, 0): 0, (-1, 0): 2, (1, 0): 3, (0, -1): 6, (0, 1): 7, (2, 0): 10, (0, 2): 11, (-1, -1): 12, (-1, 1): 13, (1, -1): 14, (1, 1): 15,
            (2, -1): 22, (2, 1): 23, (-1, 2): 24, (1, 2): 25, (2, 2): 30}
PARTNER_SLOT = {(0, 0): 1, (-1, 0): 4, (1, 0): 5, (0, -1): 8, (0, 1): 9, (2, 0): 16, (0, 2): 17, (-1, -1): 18, (-1, 1): 19, (1, -1): 20, (1, 1): 21,
                (2, -1): 26, (2, 1): 27, (-1, 2): 28, (1, 2): 29, (2, 2): 31}
RING_GROUP = {i: number for number, group in enumerate(RING_GROUPS) for i in group}
RING_SHARDS = [sum(2 if RING[i][3] is None else 1 for i in group) // 2 for group in RING_GROUPS]
PUSH_GROUPS = [PLACES[0:1], PLACES[1:3], PLACES[3:5], PLACES[5:7], PLACES[7:9], PLACES[9:11], PLACES[11:13], PLACES[13:15], PLACES[15:16]]
PUSH_GROUP = {place: number for number, group in enumerate(PUSH_GROUPS) for place in group}
N_GROUPS = len(RING_SHARDS) + len(PUSH_GROUPS)
ALL_SHARDS = sum(RING_SHARDS) + len(PLACES)


def normalized(x):
    return x * lax.rsqrt(jnp.mean(x * x, axis=-1, keepdims=True) + EPS)


def layer_kernel(n, tp, q_ref, k_ref, v_ref, cos_row, cos_col, sin_row, sin_col, qg_ref, kg_ref, og_ref, mg_ref, fg_ref,
                 ow_hbm, res_hbm, gate_hbm, up_hbm, down_hbm, out_ref,
                 keys, vals, gates, ups, dt, ow, res, att, mid, nrm, hid, part, recv, proj, proj_b, qt, s0, s1, acc, m_ref, l_ref,
                 send_sem, recv_sem, x_send, x_recv, local_sem):
    a = lax.axis_index("sp")
    t = lax.axis_index("tp")
    c = lax.rem(a, 2)
    chip = lax.div(a, 2)
    z = lax.div(chip, n)
    y = lax.rem(chip, n)
    u = y * (1 - c) + z * c
    w = z * (1 - c) + y * c
    partner = a + 1 - 2 * c

    def device_at(uu, ww, cc):
        return ((ww * (1 - cc) + uu * cc) * n + uu * (1 - cc) + ww * cc) * 2 + cc

    def own_index(du, dw):
        return device_at(lax.rem(u + du + n, n), lax.rem(w + dw + n, n), c)

    def partner_index(du, dw):
        return device_at(lax.rem(w + du + n, n), lax.rem(u + dw + n, n), 1 - c)

    neighbour = {("A", 1): own_index(1, 0), ("A", -1): own_index(-1, 0), ("B", 1): own_index(0, 1), ("B", -1): own_index(0, -1)}
    peers = [lax.rem(t + d, tp) for d in range(1, tp)]

    class Gather:
        def __init__(self, number, buffer, own, given, kept):
            self.number, self.buffer, self.own, self.given, self.kept = number, buffer, own, given, kept
            self.half_rows = buffer.shape[1] // 2

        def view(self, index, half=None):
            if half is None:
                return self.buffer.at[index]
            return self.buffer.at[index, pl.ds(half * self.half_rows, self.half_rows)]

        def copy(self, src, dst, group, target):
            return pltpu.make_async_remote_copy(
                src_ref=src, dst_ref=dst, send_sem=send_sem.at[self.number], recv_sem=recv_sem.at[self.number * N_GROUPS + group],
                device_id=(target, t), device_id_type=MESH)

        def ring(self, i):
            axis, sign, source, half, landing = RING[i]
            at = self.own(source)
            to = at if self.own is own_index_of else self.own(landing)
            return self.copy(self.view(at, half), self.view(to, half), RING_GROUP[i], neighbour[axis, sign])

        def push(self, place):
            return self.copy(self.view(self.own(place)), self.view(self.given(place)), len(RING_SHARDS) + PUSH_GROUP[place], partner)

        def shards(self, count, group):
            these = self.buffer.at[pl.ds(0, count)]
            return self.copy(these, these, group, partner)

        def stage(self, name):
            self.arrive(name)
            self.pass_on(name)

        def arrive(self, name):
            group = STAGES[name][0]
            if group is not None:
                self.shards(RING_SHARDS[group], group).wait_recv()

        def pass_on(self, name):
            _, sends, places = STAGES[name]
            for i in sends:
                self.ring(i).start()
            for place in places:
                self.push(place).start()

        def from_partner(self, *groups):
            for group in groups:
                self.shards(len(PUSH_GROUPS[group]), len(RING_SHARDS) + group).wait_recv()

        def drain(self):
            self.shards(ALL_SHARDS, 0).wait_send()

    def own_index_of(place):
        return own_index(*place)

    def chip_slot(place, core):
        return PLACES.index(place) * 2 + core

    by_slot = (OWN_SLOT.get, PARTNER_SLOT.get, PARTNER_SLOT.get)
    by_index = (own_index_of, own_index_of, lambda place: partner_index(*place))
    ks, vs = Gather(0, keys, *by_slot), Gather(1, vals, *by_slot)
    gs, us = Gather(2, gates, *by_index), Gather(3, ups, *by_index)
    downs = Gather(4, dt, lambda place: chip_slot(place, c), lambda place: chip_slot(place[::-1], c),
                   lambda place: chip_slot(place[::-1], 1 - c))

    rows = gate_hbm.shape[0]
    to_gate = pltpu.make_async_copy(gate_hbm, gates.at[a], local_sem.at[0])
    to_up = pltpu.make_async_copy(up_hbm, ups.at[a], local_sem.at[1])
    to_down = pltpu.make_async_copy(down_hbm, dt.at[chip_slot((0, 0), c)], local_sem.at[2])
    to_res = pltpu.make_async_copy(res_hbm, res.at[t], local_sem.at[3])
    to_ow = pltpu.make_async_copy(ow_hbm, ow, local_sem.at[4])
    to_res.start()
    to_gate.start()
    to_up.start()
    to_down.start()
    to_ow.start()

    barrier = pltpu.get_barrier_semaphore()
    for other in [*neighbour.values(), partner]:
        pl.semaphore_signal(barrier, inc=1, device_id=(other, t), device_id_type=MESH)
    for other in peers:
        pl.semaphore_signal(barrier, inc=1, device_id=(a, other), device_id_type=MESH)

    tok = k_ref.shape[0]
    grid_rows = tok // GRID_W

    def table(by_row, by_column):
        mine = by_row[pl.ds(a * grid_rows, grid_rows), :]
        return jnp.concatenate([mine[r:r + 1] + by_column[...] for r in range(grid_rows)], axis=0)

    cosine, sine = table(cos_row, cos_col), table(sin_row, sin_col)
    lane = lax.broadcasted_iota(jnp.int32, cosine.shape, 1)
    low = lax.rem(lax.div(lane, 32), 2) == 0

    def rotated(x, gain):
        x = normalized(x.astype(jnp.float32)) * gain
        swapped = jnp.where(low, pltpu.roll(x, 96, 1), pltpu.roll(x, 32, 1))
        return x * cosine + swapped * sine

    keys[0] = rotated(k_ref[...], kg_ref[...]).astype(jnp.bfloat16)
    for b in range(tok // 128):
        block = v_ref[b * 128:(b + 1) * 128, :].astype(jnp.float32)
        vals[0, b * 128:(b + 1) * 128, :] = block.T.astype(jnp.bfloat16)

    pl.semaphore_wait(barrier, len(neighbour) + 1 + len(peers))
    ks.stage("1A")
    vs.stage("1A")

    def x_copy(src, dst, kind, group, other):
        return pltpu.make_async_remote_copy(src_ref=src, dst_ref=dst, send_sem=x_send.at[kind], recv_sem=x_recv.at[group],
                                            device_id=(a, other), device_id_type=MESH)

    def res_copy(d):
        return x_copy(res.at[t], res.at[t], 0, 0, lax.rem(t + d, tp))

    def att_copy(block, d):
        return x_copy(att.at[block, t], att.at[block, t], 1, 1 + block, lax.rem(t + d, tp))

    def part_copy(half, column, d):
        other = lax.rem(t + d, tp)
        return x_copy(part.at[half, column, other], recv.at[half, column, d - 1], 2 + half, 5 + half * part.shape[1] + column, other)

    def x_all(these, kind, group):
        return x_copy(these, these, kind, group, lax.rem(t + 1, tp))

    to_res.wait()
    for d in range(1, tp):
        res_copy(d).start()

    heads = q_ref.shape[1] // 128
    blocks = tok // 128
    part_rows = 128 // tp
    for h in range(heads):
        rot = rotated(q_ref[:, h * 128:(h + 1) * 128], qg_ref[...]).astype(jnp.bfloat16)
        scaled = rot.astype(jnp.float32) * LOG2_SCALE
        for b in range(blocks):
            turned = jnp.concatenate([scaled[o * 128 + b * part_rows:o * 128 + (b + 1) * part_rows] for o in range(tp)], axis=0).T
            high = turned.astype(jnp.bfloat16)
            at = (b * heads + h) * 128
            qt[0:128, at:at + 128] = high
            qt[128:256, at:at + 128] = (turned - high.astype(jnp.float32)).astype(jnp.bfloat16)

    m_ref[...] = jnp.full_like(m_ref, -1e30)
    l_ref[...] = jnp.zeros_like(l_ref)
    acc[...] = jnp.zeros_like(acc)

    buffers = [s0, s1]

    def columns(j):
        return pl.ds(pl.multiple_of(j * UNIT, UNIT), UNIT)

    def score(chunk, j, into):
        rows_in = keys[pl.ds(chunk * 2, 2)].reshape(2 * tok, 128)
        into[...] = jnp.dot(jnp.concatenate([rows_in, rows_in], axis=1), qt[:, columns(j)], preferred_element_type=jnp.float32)

    def absorb(chunk, j, held):
        turned = jnp.concatenate(
            [vals[chunk * 2 + h, b * 128:(b + 1) * 128, :] for h in range(2) for b in range(blocks)], axis=1)
        at = columns(j)
        scores = held[...]
        before = m_ref[:, at]
        highest = jnp.maximum(before, jnp.max(scores, axis=0, keepdims=True))
        weights = jnp.exp2(scores - highest)
        factor = jnp.exp2(before - highest)
        m_ref[:, at] = highest
        l_ref[:, at] = l_ref[:, at] * factor + jnp.sum(weights, axis=0, keepdims=True)
        acc[:, at] = acc[:, at] * factor + jnp.dot(turned, weights.astype(jnp.bfloat16), preferred_element_type=jnp.float32)

    def both(*groups):
        for gather in (ks, vs):
            gather.from_partner(*groups)

    events = {
        (0, 2): [lambda: ks.stage("1B"), lambda: vs.stage("1B"), lambda: to_down.wait(), lambda: downs.stage("1A"), lambda: ks.stage("2A")],
        (1, 0): [lambda: vs.arrive("2A")],
        (1, 2): [lambda: ks.stage("2B"), lambda: vs.pass_on("2A"), lambda: both(1)],
        (2, 2): [lambda: vs.stage("2B")],
        (3, 2): [lambda: both(2)],
        (4, 0): [lambda: ks.stage("3"), lambda: to_gate.wait(), lambda: gs.stage("1A")],
        (4, 2): [lambda: vs.stage("3")],
        (5, 2): [lambda: gs.stage("1B")],
        (6, 2): [lambda: ks.stage("4"), lambda: to_up.wait(), lambda: us.stage("1A")],
        (7, 2): [lambda: both(3)],
    }
    ks.from_partner(0)
    score(0, 0, s0)
    vs.from_partner(0)
    n_units = blocks * heads * 128 // UNIT

    def run(table, index, *unit):
        for at, todo in table.items():
            if at[1:] == unit:
                @pl.when(index == at[0])
                def _():
                    for event in todo:
                        event()

    def first_phase(k, carry):
        for j in range(n_units):
            if j % 2 == 0:
                run(events, k, j)
            if j + 1 < n_units:
                score(k, j + 1, buffers[(j + 1) % 2])
            else:
                score(k + 1, 0, buffers[0])
            absorb(k, j, buffers[j % 2])
        return carry

    lax.fori_loop(0, PHASE1, first_phase, 0)

    last = keys.shape[0] // 2
    later = {
        (0, 8): [lambda: vs.stage("4"), lambda: both(4, 5), lambda: us.stage("1B")],
        (0, 10): [lambda: gs.stage("2A"), lambda: gs.stage("2B")],
        (0, 12): [lambda: both(6, 7), lambda: ks.stage("5")],
        (0, 14): [lambda: vs.stage("5"), lambda: both(8)],
        (1, 10): [lambda: us.stage("2A"), lambda: us.stage("2B")],
        (2, 8): [lambda: gs.stage("3")],
        (3, 8): [lambda: us.stage("3")],
        (3, 14): [lambda: gs.stage("4"), lambda: downs.stage("1B")],
    }

    def second_phase(j, carry):
        for k in range(PHASE1, last):
            i = k - PHASE1
            if i % 2 == 0:
                run(later, j, k)
            if k + 1 < last:
                score(k + 1, j, buffers[(i + 1) % 2])
            else:
                score(PHASE1, lax.rem(j + 1, n_units), buffers[(i + 1) % 2])
            absorb(k, j, buffers[i % 2])
        at = columns(j)
        mixed = acc[:, at] / l_ref[:, at]
        for h in range(heads):
            att[j, t, :, h * 128:(h + 1) * 128] = mixed[:, h * 128:(h + 1) * 128].T.astype(jnp.bfloat16)
        for d in range(1, tp):
            att_copy(j, d).start()
        return carry

    lax.fori_loop(0, n_units, second_phase, 0)

    to_ow.wait()
    x_all(res.at[pl.ds(0, tp - 1)], 0, 0).wait_recv()


    quarters = 4
    width_part = ow.shape[1] // quarters

    def dots(b, into, i):
        rows_in = jnp.concatenate([att[b, s] for s in range(tp)], axis=1)
        at = slice(i * width_part, (i + 1) * width_part)
        into[:, at] = jnp.dot(rows_in, ow[:, at], preferred_element_type=jnp.float32)

    def norms(b, held, i):
        mine = slice(b * part_rows, (b + 1) * part_rows)
        at = slice(i * part_rows, (i + 1) * part_rows)
        stream = (res[i, mine, :].astype(jnp.float32) + og_ref[...] * normalized(held[at, :])).astype(jnp.bfloat16)
        mid[i, mine, :] = stream
        nrm[b * 128 + i * part_rows:b * 128 + (i + 1) * part_rows, :] = (
            mg_ref[...] * normalized(stream.astype(jnp.float32))).astype(jnp.bfloat16)

    half_rows = tok // 2

    projected = [proj, proj_b]

    def project(first, count, after):
        for b in range(first, first + count + 1):
            now = b < first + count
            if now:
                x_all(att.at[b, pl.ds(0, tp - 1)], 1, 1 + b).wait_recv()
            for i in range(quarters):
                if now:
                    dots(b, projected[b % 2], i)
                if b > first:
                    norms(b - 1, projected[(b - 1) % 2], i)
            for event in after.get((b,), []):
                event()

    width = gates.shape[0] * rows
    n_hidden = gates.shape[2] // 128

    def feed(half, first, last_one):
        these = slice(half * half_rows, (half + 1) * half_rows)

        def gated_dot(i, into):
            at = pl.ds(pl.multiple_of(i * 128, 128), 128)
            pair = jnp.concatenate([gates[:, :, at].reshape(width, 128), ups[:, :, at].reshape(width, 128)], axis=1)
            into[0:half_rows, 0:256] = jnp.dot(nrm[these, :], pair, preferred_element_type=jnp.float32)

        def gating(i, held):
            gate, up = held[0:half_rows, 0:128], held[0:half_rows, 128:256]
            hid[these, pl.ds(pl.multiple_of(i * 128, 128), 128)] = (gate / (1.0 + jnp.exp(-gate)) * up).astype(jnp.bfloat16)

        gated_dot(first, s0)
        pairs = (last_one - first - 1) // 2

        def hidden_pair(i, carry):
            at = first + 2 * i
            gated_dot(at + 1, s1)
            gating(at, s0)
            gated_dot(at + 2, s0)
            gating(at + 1, s1)
            return carry

        lax.fori_loop(0, pairs, hidden_pair, 0)
        at = first + 2 * pairs
        if at + 1 < last_one:
            gated_dot(at + 1, s1)
            gating(at, s0)
            gating(at + 1, s1)
        else:
            gating(at, s0)

    per_block = 256 // rows
    n_columns = dt.shape[0] // per_block
    owned = half_rows // tp

    def shrink(half, first, count, before):
        these = slice(half * half_rows, (half + 1) * half_rows)

        def down_block(i, carry):
            run(before, i)
            weight = dt[pl.ds(i * per_block, per_block)].reshape(256, dt.shape[2])
            share = lax.dot_general(hid[these, :], weight, (((1,), (1,)), ((), ())), preferred_element_type=jnp.float32).astype(jnp.bfloat16)
            for o in range(tp):
                part[half, i, o] = jnp.concatenate(
                    [share[b * 128 + o * part_rows:b * 128 + (o + 1) * part_rows] for b in range(blocks // 2)], axis=0)

            @pl.when(i > first)
            def _():
                for d in range(1, tp):
                    part_copy(half, i - 1, d).start()
            return carry

        lax.fori_loop(first, first + count, down_block, 0)
        for d in range(1, tp):
            part_copy(half, first + count - 1, d).start()

    project(0, blocks - 1, {(0,): [lambda: us.stage("4"), lambda: downs.stage("2A")],
                        (2,): [lambda: downs.stage("2B"), lambda: gs.stage("5")],
                        (3,): [lambda: us.stage("5")]})
    for gather in (gs, us):
        gather.from_partner(*range(len(PUSH_GROUPS)))
    feed(0, 0, n_hidden)
    downs.from_partner(0, 1, 2)
    shrink(0, 0, 1, {})
    shrink(0, 1, 1, {})
    downs.stage("3")
    project(blocks - 1, 1, {})
    downs.from_partner(3, 4, 5)
    shrink(0, 2, 3, {})
    feed(1, 0, n_hidden)
    shrink(1, 0, 1, {})
    shrink(1, 1, 1, {})
    downs.stage("4")
    shrink(1, 2, 3, {})
    downs.from_partner(6, 7)
    downs.stage("5")
    shrink(0, 5, 2, {})
    shrink(1, 5, 2, {})
    downs.from_partner(8)
    shrink(0, 7, 1, {})
    shrink(1, 7, 1, {})

    for half, columns_of in ((0, range(5)), (1, range(5)), (0, [5, 6]), (1, [5, 6]), (0, [7]), (1, [7])):
        for i in columns_of:
            x_all(recv.at[half, i], 2, 5 + half * n_columns + i).wait_recv()
            total = part[half, i, t].astype(jnp.float32)
            for d in range(tp - 1):
                total = total + recv[half, i, d].astype(jnp.float32)
            for h in range(2):
                chip_at = lax.div(own_index(*PLACES[2 * i + h]), 2)
                proj[half * owned:(half + 1) * owned, pl.ds(pl.multiple_of(chip_at * 128, 128), 128)] = total[:, h * 128:(h + 1) * 128]

    def finish(i, carry):
        at = pl.ds(pl.multiple_of(i * 32, 32), 32)
        out_ref[at, :] = (mid[t, at, :].astype(jnp.float32) + fg_ref[...] * normalized(proj[at, :])).astype(jnp.bfloat16)
        return carry

    lax.fori_loop(0, 4, finish, 0)

    for gather in (ks, vs, gs, us, downs):
        gather.drain()
    x_all(res.at[pl.ds(0, tp - 1)], 0, 0).wait_send()
    x_all(att.at[pl.ds(0, tp - 1)], 1, 0).wait_send()
    for half in range(2):
        x_all(part.at[half, pl.ds(0, n_columns * (tp - 1) // tp)], 2 + half, 0).wait_send()


def on_device(queries, keys, values, q_gain, k_gain, out_weight, out_gain, residual_in, mlp_gain, gate_weight, up_weight, down_weight, final_gain):
    sp, tp = lax.axis_size("sp"), lax.axis_size("tp")
    n = math.isqrt(sp // 2)
    tok, head = keys.shape
    rows, hidden = gate_weight.shape
    width = out_weight.shape[1]
    quarter = head // 4
    freqs = np.float32(10000.0) ** (-np.arange(quarter, dtype=np.float32) / np.float32(quarter))

    def table(function, signs, count, low):
        angle = np.arange(count, dtype=np.float32)[:, None] * freqs
        values, empty = function(angle.astype(np.float64)).astype(np.float32), np.zeros((count, 2 * quarter), np.float32)
        turned = np.concatenate([signs[0] * values, signs[1] * values], axis=1)
        return jnp.asarray(np.concatenate([turned, empty] if low else [empty, turned], axis=1).astype(np.float32))

    tables = [table(function, signs, count, low) for function, signs in ((np.cos, (1.0, 1.0)), (np.sin, (-1.0, 1.0)))
              for count, low in ((sp * tok // GRID_W, True), (GRID_W, False))]
    blocks = tok // 128
    bf16, f32 = jnp.bfloat16, jnp.float32
    vmem = pl.BlockSpec(memory_space=pltpu.VMEM)
    anywhere = pl.BlockSpec(memory_space=pl.ANY)
    n_columns = width // 256
    q_columns = tok * queries.shape[1] // head
    return pl.pallas_call(
        functools.partial(layer_kernel, n, tp),
        out_shape=jax.ShapeDtypeStruct(residual_in.shape, bf16),
        in_specs=[vmem] * 12 + [anywhere] * 5,
        out_specs=vmem,
        scratch_shapes=[
            pltpu.VMEM((sp, tok, head), bf16),
            pltpu.VMEM((sp, tok, head), bf16),
            pltpu.VMEM((sp, rows, hidden), bf16),
            pltpu.VMEM((sp, rows, hidden), bf16),
            pltpu.VMEM((sp, rows, hidden), bf16),
            pltpu.VMEM(out_weight.shape, bf16),
            pltpu.VMEM((tp, *residual_in.shape), bf16),
            pltpu.VMEM((blocks, tp, 128, queries.shape[1]), bf16),
            pltpu.VMEM((blocks, 128, width), bf16),
            pltpu.VMEM((tok, width), bf16),
            pltpu.VMEM((tok, hidden), bf16),
            pltpu.VMEM((2, n_columns, tp, 64, 256), bf16),
            pltpu.VMEM((2, n_columns, tp - 1, 64, 256), bf16),
            pltpu.VMEM((128, width), f32),
            pltpu.VMEM((128, width), f32),
            pltpu.VMEM((2 * head, q_columns), bf16),
            pltpu.VMEM((2 * tok, UNIT), f32),
            pltpu.VMEM((2 * tok, UNIT), f32),
            pltpu.VMEM((head, q_columns), f32),
            pltpu.VMEM((1, q_columns), f32),
            pltpu.VMEM((1, q_columns), f32),
            pltpu.SemaphoreType.DMA((5,)),
            pltpu.SemaphoreType.DMA((5 * N_GROUPS,)),
            pltpu.SemaphoreType.DMA((4,)),
            pltpu.SemaphoreType.DMA((5 + 2 * n_columns,)),
            pltpu.SemaphoreType.DMA((5,)),
        ],
        compiler_params=pltpu.CompilerParams(collective_id=0, has_side_effects=True, vmem_limit_bytes=67043328),
        name="layer",
    )(queries, keys, values, *tables,
      q_gain[None], k_gain[None], out_gain[None], mlp_gain[None], final_gain[None],
      out_weight, residual_in, gate_weight, up_weight, down_weight.T)


def solution(mesh):
    return jax.shard_map(
        on_device,
        mesh=mesh,
        in_specs=(
            P("sp", "tp"), P("sp", "tp"), P("sp", "tp"), P(), P(), P(), P(), P(("sp", "tp"), None), P(),
            P("sp", "tp"), P("sp", "tp"), P("tp", "sp"), P(),
        ),
        out_specs=P(("sp", "tp"), None),
        check_vma=False,
    )
```
